32 devices in a mesh: sp: 8 (over z, core), tp: 4 (over y, x).
Axes of the slice: x: 2, y: 2, z: 4, core: 2. Of those that a mesh axis runs over, the one named last changes fastest.
Arguments:
- mix_values: bfloat16 [1024, 4096], P('sp', 'tp'), may hold values from -6 to 6
- mix_gate: bfloat16 [1024, 4096], P('sp', 'tp'), may hold values from -6 to 6
- input_keys: bfloat16 [1024, 2048], P('sp', 'tp'), may hold values from -0.31640625 to 0.31640625
- output_keys: bfloat16 [1024, 2048], P('sp', 'tp'), may hold values from -0.31640625 to 0.31640625
- step_sizes: float32 [1024, 64], P('sp', 'tp'), may hold values from 0.1 to 8
- decay_rates: float32 [64], P('tp'), may hold values from 4.8828125e-05 to 0.03
- out_proj: bfloat16 [2048, 4096], P('sp', 'tp'), may hold values from -0.09375 to 0.09375
- expert_inputs: bfloat16 [1024, 2048], P('sp'), may hold values from -20 to 20
- stream_grad: bfloat16 [1024, 2048], P('sp'), may hold values from -6 to 6
- routes: int32 [1024, 2], P('sp'), may hold values from 0 to 7, all different within a row; in each aligned block of 128 rows (0 to 127, 128 to 255, ...) at most 48 rows name the same one
- route_weights: float32 [1024, 2], P('sp'), may hold values from 0.1 to 0.9
- gate_proj: bfloat16 [8, 2048, 2048], P('sp', 'tp'), may hold values from -0.125 to 0.125
- up_proj: bfloat16 [8, 2048, 2048], P('sp', 'tp'), may hold values from -0.125 to 0.125
- down_proj: bfloat16 [8, 2048, 2048], P('sp', 'tp'), may hold values from -0.125 to 0.125
Outputs:
- grad_gate_proj: bfloat16 [8, 2048, 2048], P('sp', 'tp')
- grad_up_proj: bfloat16 [8, 2048, 2048], P('sp', 'tp')
- grad_down_proj: bfloat16 [8, 2048, 2048], P('sp', 'tp')
- grad_out_proj: float32 [2048, 4096], P('sp', 'tp')
- grad_values: bfloat16 [1024, 4096], P('sp', 'tp')
- grad_gate: bfloat16 [1024, 4096], P('sp', 'tp')
- grad_input_keys: bfloat16 [1024, 2048], P('sp', 'tp')
- grad_output_keys: bfloat16 [1024, 2048], P('sp', 'tp')
- grad_steps: float32 [1024, 64], P('sp', 'tp')
The draws below stay inside these ranges and needn't reach their ends.
Inputs may be any that keep to these rules, and one draw needn't show every extreme that they name: In the rows of one device no expert is named by more than 48 routes, and on some devices one expert is named by exactly 48; the 2 routes of a token name different experts.
All inputs are finite; a program needn't handle non-finite values.
Results may differ from the reference program's by a relative error of at most 0.025.
Values may be sent and summed in bfloat16 or wider, within the bound.
A program may use at most 64 MiB of HBM per device.

```python
import math
import jax
import jax.numpy as jnp
import numpy as np
from jax import lax

D = 2048
HEAD_DIM = 64
HEADS = 64
GROUPS = 16
NSTATE = 128
BLOCK = 128
F = 2048
TOPK = 2
TOK_DEV = 128
DI = 4096
EXPERTS = 8
TOKENS = 1024
CAP = 48
N_SP = 8


def draw_decay_rates(key, part):
    choose_key, fast_key, slow_key = jax.random.split(jax.random.fold_in(key, 11), 3)
    share = 0.5
    fast_heads = jax.random.uniform(choose_key, (HEADS,), jnp.float32) < share
    fast_rate = jnp.exp(jax.random.uniform(fast_key, (HEADS,), jnp.float32, jnp.log(0.01), jnp.log(0.03)))
    slow_rate = jnp.exp(jax.random.uniform(slow_key, (HEADS,), jnp.float32, jnp.log(0.05), jnp.log(0.5))) / TOKENS
    return jnp.where(fast_heads, fast_rate, slow_rate).astype(jnp.float32)


def draw_step_sizes(key, part):
    base_key, block_key = jax.random.split(jax.random.fold_in(key, 23), 2)
    base = jnp.exp(jax.random.uniform(base_key, (TOKENS, HEADS), jnp.float32, -0.7, 0.7))
    factor = jnp.exp(jax.random.uniform(block_key, (TOKENS // BLOCK, 1), jnp.float32, jnp.log(0.4), jnp.log(2.5)))
    return (base * jnp.repeat(factor, BLOCK, axis=0)).astype(jnp.float32)


def draw_expert_inputs(key, part):
    base_key, pick_key, scale_key = jax.random.split(jax.random.fold_in(key, 37), 3)
    base = jnp.clip(jax.random.normal(base_key, (TOKENS, D), jnp.float32), -2.5, 2.5)
    picked = jax.random.uniform(pick_key, (TOKENS, 1), jnp.float32) < 0.0625
    row_scale = jax.random.uniform(scale_key, (TOKENS, 1), jnp.float32, 5.0, 8.0)
    return (base * jnp.where(picked, row_scale, 1.0)).astype(jnp.bfloat16)


def with_spikes(array, key, source, target, parts, factor):
    owner, partner = [(jnp.arange(array.shape[axis_at]) // (array.shape[axis_at] // parts)).reshape([-1 if axis == axis_at else 1 for axis in range(array.ndim)]) for axis_at in (source, target)]
    chosen = jax.random.permutation(key, parts)[partner]
    strong = (owner == chosen) | (owner == (partner + parts // 2) % parts)
    return jnp.where(strong, factor * array, array)


def levels(stream_key, dims, cuts, low, top_value):
    def one(position, parts):
        heights = jax.random.uniform(jax.random.fold_in(jax.random.fold_in(stream_key, 6), position), (parts,), jnp.float32, low / len(cuts), top_value / len(cuts))
        return jnp.repeat(jnp.exp(heights), dims[position] // parts).reshape((-1,) + (1,) * (len(dims) - position - 1))

    loudness = one(*cuts[0])
    for cut in cuts[1:]:
        loudness = loudness * one(*cut)
    return loudness


def assign_block(rng, own, number, rows, number_of, top, bound, skew):
    sequence = jax.random.permutation(rng, number_of)
    crowded, usual = shares(number_of, rows * top, bound, skew, True), shares(number_of, rows * top, bound, skew, False)
    places = jnp.arange(number_of)

    def named(lengths, turn):
        used = int((lengths > 0).sum())
        fixed = max(1, used // 4)
        moved = fixed + (places - fixed + turn * (used - fixed)) % max(1, number_of - fixed)
        return jnp.zeros((number_of,), jnp.int32).at[sequence[jnp.where(places < fixed, places, moved)]].set(jnp.asarray(lengths, jnp.int32))

    lengths = jnp.where(number % 4 == 0, named(crowded, number // 4), named(usual, number - number // 4 - 1))
    mixed = jax.random.permutation(jax.random.fold_in(own, 3), number_of)
    donor, receiver = mixed[0:number_of // 2 * 2:2], mixed[1:number_of // 2 * 2:2]
    room = jnp.minimum(lengths[donor] - 1, bound - lengths[receiver]) // 2
    room = jnp.where((donor == sequence[0]) | (receiver == sequence[0]) | (lengths[receiver] == 0), 0, jnp.maximum(room, 0))
    moved = jax.random.randint(jax.random.fold_in(own, 4), (number_of // 2,), 0, 1 << 20) % (room + 1)
    lengths = lengths.at[donor].add(-moved).at[receiver].add(moved)
    members = jnp.searchsorted(jnp.cumsum(lengths), jnp.arange(rows * top), side="right").astype(jnp.int32)
    table = members.reshape(top, rows).T
    table = table[jax.random.permutation(jax.random.fold_in(own, 1), rows)]
    turn = jax.random.randint(jax.random.fold_in(own, 2), (rows, 1), 0, top)
    return jnp.take_along_axis(table, (jnp.arange(top)[None, :] + turn) % top, axis=1)


def shares(count, total, most, lean, full):
    weights = [(1 << 20) // math.isqrt(standing ** lean) + 1 for standing in range(1, count + 1)]
    largest = most if full else min(most, max(-(-total // count), total * weights[0] // sum(weights)))
    least = 1 if total - largest >= count - 1 else 0
    given, spare = [largest] + [least] * (count - 1), total - largest - least * (count - 1)
    while spare > 0:
        free = [i for i in range(1, count) if given[i] < largest] or [i for i in range(1, count) if given[i] < most]
        pool, budget = sum([weights[i] for i in free]), spare
        for i in free:
            addition = min(most - given[i], max(1, budget * weights[i] // pool), spare)
            given[i] = given[i] + addition
            spare = spare - addition
    return np.array(given)


def gaussian(stream_key, dims, width, limit, shards=(), held_as=jnp.bfloat16):
    factor_of = levels(stream_key, dims, shards, -0.22, 0.18) if shards else 1.0
    result = jax.random.normal(stream_key, dims, jnp.float32) * width * factor_of
    return jnp.minimum(jnp.maximum(result, -limit), limit).astype(held_as)


def heavy_noise(own_key, shape, width, most, cuts, heavy, kind=jnp.bfloat16):
    array = width * jax.random.normal(own_key, shape, jnp.float32)
    if cuts:
        array = array * levels(own_key, shape, cuts, -0.22, 0.18)
    return jnp.clip(with_spikes(array, jax.random.fold_in(own_key, 3), *heavy), -most, most).astype(kind)


def setup_inputs(seed: int = 0) -> dict:
    key_of = jax.random.split(jax.random.key(seed), 15)
    mix_values = gaussian(key_of[0], (TOKENS, DI), 1.0, 6.0, ((0, 8), (1, 4)))
    mix_gate = gaussian(key_of[1], (TOKENS, DI), 1.0, 6.0, ((0, 8), (1, 4)))
    input_keys = gaussian(key_of[2], (TOKENS, GROUPS * NSTATE), (0.3 * TOKENS ** -0.25), 0.31640625, ((0, 8), (1, 4)))
    output_keys = gaussian(key_of[3], (TOKENS, GROUPS * NSTATE), (0.3 * TOKENS ** -0.25), 0.31640625, ((0, 8), (1, 4)))
    step_sizes = draw_step_sizes(jax.random.fold_in(key_of[14], 71), 0)
    decay_rates = draw_decay_rates(jax.random.fold_in(key_of[14], 71), 0)
    out_proj = gaussian(key_of[6], (D, DI), DI ** -0.5, 0.09375, ((0, 8), (1, 4)))
    expert_inputs = draw_expert_inputs(jax.random.fold_in(key_of[14], 71), 0)
    stream_grad = heavy_noise(key_of[8], (TOKENS, D), 1.0, 6.0, ((0, 8),), (0, 1, 8, 2.0))
    routes_keys = jax.random.split(jax.random.fold_in(key_of[9], 1), TOKENS // TOK_DEV)
    routes_turns = jax.random.permutation(jax.random.fold_in(key_of[9], 3), TOKENS // TOK_DEV)
    routes = jax.vmap(lambda own, number: assign_block(jax.random.fold_in(key_of[9], 2), own, number, TOK_DEV, EXPERTS, TOPK, CAP, 1))(routes_keys, routes_turns).reshape((TOKENS, TOPK))
    route_weights = jnp.clip(0.1 + 0.79999997 * jax.random.uniform(key_of[10], (TOKENS, TOPK), jnp.float32) ** levels(key_of[10], (TOKENS, TOPK), ((0, 8),), -0.2, 0.2), 0.1, 0.9)
    gate_proj = gaussian(key_of[11], (EXPERTS, F, D), D ** -0.5, 0.125, ((0, 8), (1, 4)))
    up_proj = gaussian(key_of[12], (EXPERTS, F, D), D ** -0.5, 0.125, ((0, 8), (1, 4)))
    down_proj = gaussian(key_of[13], (EXPERTS, F, D), F ** -0.5, 0.125, ((0, 8), (1, 4)))
    return dict(mix_values=mix_values, mix_gate=mix_gate, input_keys=input_keys, output_keys=output_keys, step_sizes=step_sizes, decay_rates=decay_rates, out_proj=out_proj, expert_inputs=expert_inputs, stream_grad=stream_grad, routes=routes, route_weights=route_weights, gate_proj=gate_proj, up_proj=up_proj, down_proj=down_proj)


CLAMP_LIMIT = 7.0
SIGMOID_SCALE = 1.702
HIGHEST = lax.Precision.HIGHEST

def decay_span(head_values, in_keys, out_keys, head_steps, head_rates, start_state):
    length = head_values.shape[0]
    num_blocks = length // BLOCK
    causal_mask = jnp.tril(jnp.ones((BLOCK, BLOCK), dtype=bool))

    def advance(carry_state, block_data):
        block_values, block_in, block_out, block_steps = block_data
        log_decay = jnp.cumsum(-block_steps * head_rates, axis=0)
        weighted = block_values * block_steps[..., None]
        ordered = jnp.transpose(log_decay, (1, 2, 0))
        log_gaps = ordered[..., :, None] - ordered[..., None, :]
        mixing = jnp.where(causal_mask, jnp.exp(jnp.where(causal_mask, log_gaps, 0.0)), 0.0)
        scores = jnp.einsum('lgn,sgn->gls', block_out, block_in, precision=HIGHEST)
        within = jnp.einsum('grls,sgrp->lgrp', scores[:, None] * mixing, weighted, precision=HIGHEST)
        carried = jnp.einsum('lgn,grpn->lgrp', block_out, carry_state, precision=HIGHEST) * jnp.exp(log_decay)[..., None]
        to_end = jnp.exp(log_decay[-1] - log_decay)
        new_state = carry_state * jnp.exp(log_decay[-1])[..., None, None] + jnp.einsum('lgn,lgrp->grpn', block_in, weighted * to_end[..., None], precision=HIGHEST)
        return (new_state, within + carried)
    blocks = tuple((whole_array.reshape((num_blocks, BLOCK) + whole_array.shape[1:]) for whole_array in (head_values, in_keys, out_keys, head_steps)))
    last_state, block_outputs = lax.scan(advance, start_state, blocks)
    return (block_outputs.reshape(head_values.shape), last_state)

def expert_backward(in_rows, grad_rows, gate_weight, up_weight, down_weight):
    contract = (((1,), (1,)), ((), ()))
    across = (((0,), (0,)), ((), ()))
    gate_pre = lax.dot_general(in_rows, gate_weight, contract, preferred_element_type=jnp.float32)
    up_pre = lax.dot_general(in_rows, up_weight, contract, preferred_element_type=jnp.float32)
    gate_clamped = jnp.minimum(gate_pre, CLAMP_LIMIT)
    up_clamped = jnp.clip(up_pre, -CLAMP_LIMIT, CLAMP_LIMIT)
    gate_sigmoid = jax.nn.sigmoid(SIGMOID_SCALE * gate_clamped)
    activation = ((up_clamped + 1.0) * gate_clamped * gate_sigmoid).astype(jnp.bfloat16)
    act_grad = lax.dot_general(grad_rows, down_weight, contract, preferred_element_type=jnp.float32)
    gate_grad = jnp.where(gate_pre < CLAMP_LIMIT, act_grad * (up_clamped + 1.0) * gate_sigmoid * (1.0 + SIGMOID_SCALE * gate_clamped * (1.0 - gate_sigmoid)), 0.0).astype(jnp.bfloat16)
    up_grad = jnp.where(jnp.abs(up_pre) < CLAMP_LIMIT, act_grad * gate_clamped * gate_sigmoid, 0.0).astype(jnp.bfloat16)
    grad_down = lax.dot_general(activation, grad_rows, across, preferred_element_type=jnp.float32).astype(jnp.bfloat16)
    grad_gate_w = lax.dot_general(gate_grad, in_rows, across, preferred_element_type=jnp.float32).astype(jnp.bfloat16)
    grad_up_w = lax.dot_general(up_grad, in_rows, across, preferred_element_type=jnp.float32).astype(jnp.bfloat16)
    input_grad = jnp.dot(gate_grad, gate_weight, preferred_element_type=jnp.float32) + jnp.dot(up_grad, up_weight, preferred_element_type=jnp.float32)
    return (grad_gate_w, grad_up_w, grad_down, input_grad)

def reference(mix_values, mix_gate, input_keys, output_keys, step_sizes, decay_rates, out_proj, expert_inputs, stream_grad, routes, route_weights, gate_proj, up_proj, down_proj):
    per_group = HEADS // GROUPS
    head_values = mix_values.astype(jnp.float32).reshape(TOKENS, GROUPS, per_group, HEAD_DIM)
    in_keys = input_keys.astype(jnp.float32).reshape(TOKENS, GROUPS, NSTATE)
    out_keys = output_keys.astype(jnp.float32).reshape(TOKENS, GROUPS, NSTATE)
    head_steps = step_sizes.reshape(TOKENS, GROUPS, per_group)
    head_rates = decay_rates.reshape(GROUPS, per_group)
    start_state = jnp.zeros((GROUPS, per_group, HEAD_DIM, NSTATE), jnp.float32)

    def mixer_only(values_in, keys_in, keys_out, steps_in):
        return decay_span(values_in, keys_in, keys_out, steps_in, head_rates, start_state)[0]
    mixer_out, back_mixer = jax.vjp(mixer_only, head_values, in_keys, out_keys, head_steps)
    gate_in = mix_gate.astype(jnp.float32).reshape(TOKENS, GROUPS, per_group, HEAD_DIM)
    gate_sigmoid = jax.nn.sigmoid(gate_in)
    gate_silu = gate_in * gate_sigmoid
    gated_out = (mixer_out * gate_silu).reshape(TOKENS, DI).astype(jnp.bfloat16)
    flat_routes = routes.reshape(-1)
    one_hot = (flat_routes[:, None] == jnp.arange(EXPERTS, dtype=jnp.int32)[None, :]).astype(jnp.int32)
    slot_rank = lax.optimization_barrier(jnp.sum((jnp.cumsum(one_hot, axis=0) - 1) * one_hot, axis=1))
    expert_slots = N_SP * CAP
    slot_index = (flat_routes * expert_slots + slot_rank).astype(jnp.int32)
    slot_table = jnp.zeros((EXPERTS * expert_slots,), jnp.int32).at[slot_index].set(jnp.arange(TOKENS * TOPK, dtype=jnp.int32) + 1)
    flat_weights = route_weights.reshape(-1)

    def expert_pass(packed):
        slot_routes, gate_weight, up_weight, down_weight = packed
        slot_used = slot_routes > 0
        route_id = jnp.maximum(slot_routes - 1, 0)
        token_id = route_id // TOPK
        route_scale = jnp.where(slot_used, flat_weights[route_id], 0.0)
        grad_rows = (stream_grad[token_id].astype(jnp.float32) * route_scale[:, None]).astype(jnp.bfloat16)
        in_rows = jnp.where(slot_used[:, None], expert_inputs[token_id], jnp.zeros((), jnp.bfloat16))
        return expert_backward(in_rows, grad_rows, gate_weight, up_weight, down_weight)
    grad_gate_proj, grad_up_proj, grad_down_proj, input_grads = lax.map(expert_pass, (slot_table.reshape(EXPERTS, expert_slots), gate_proj, up_proj, down_proj))
    per_route = input_grads.reshape(EXPERTS * expert_slots, D)[slot_index].reshape(TOKENS, TOPK, D)
    stream_total = (stream_grad.astype(jnp.float32) + lax.optimization_barrier(jnp.sum(per_route, axis=1))).astype(jnp.bfloat16)
    across = (((0,), (0,)), ((), ()))
    grad_out_proj = lax.dot_general(stream_total, gated_out, across, preferred_element_type=jnp.float32)
    gated_grad = jnp.dot(stream_total, out_proj, preferred_element_type=jnp.float32).reshape(TOKENS, GROUPS, per_group, HEAD_DIM)
    grad_gate = (gated_grad * mixer_out * gate_sigmoid * (1.0 + gate_in * (1.0 - gate_sigmoid))).reshape(TOKENS, DI).astype(jnp.bfloat16)
    mixer_grad = gated_grad * gate_silu
    grad_vals, grad_in, grad_out, grad_step = back_mixer(mixer_grad)
    return (grad_gate_proj, grad_up_proj, grad_down_proj, grad_out_proj, grad_vals.reshape(TOKENS, DI).astype(jnp.bfloat16), grad_gate, grad_in.reshape(TOKENS, GROUPS * NSTATE).astype(jnp.bfloat16), grad_out.reshape(TOKENS, GROUPS * NSTATE).astype(jnp.bfloat16), grad_step.reshape(TOKENS, HEADS))
```

```python
import functools

import jax
import jax.numpy as jnp
from jax import lax
from jax.experimental import pallas as pl
from jax.experimental.pallas import tpu as pltpu
from jax.sharding import PartitionSpec as P

NSTATE = 128
CLAMP_LIMIT = 7.0
SIGMOID_SCALE = 1.702
HIGHEST = lax.Precision.HIGHEST
F32 = jnp.float32
BF16 = jnp.bfloat16
NN = (((1,), (0,)), ((), ()))
NT = (((1,), (1,)), ((), ()))
TN = (((0,), (0,)), ((), ()))
MESH = pl.DeviceIdType.MESH


def mm(a, b, dims=NN):
    return lax.dot_general(a, b, dims, preferred_element_type=F32)


def mm_exact(a, b, dims=NN):
    return lax.dot_general(a, b, dims, precision=HIGHEST, preferred_element_type=F32)


def grid_of(rows, cols):
    return (
        lax.broadcasted_iota(jnp.int32, (rows, cols), 0),
        lax.broadcasted_iota(jnp.int32, (rows, cols), 1),
    )


def spread(heads, size):
    at, col = grid_of(heads, heads * size)
    return ((col >= at * size) & (col < (at + 1) * size)).astype(F32)


def fold(heads, size):
    col, at = grid_of(heads * size, heads)
    return ((col >= at * size) & (col < (at + 1) * size)).astype(F32)


def out(shape, dtype):
    return jax.ShapeDtypeStruct(shape, dtype)


def mixing_of(log_ref, logt_ref, h):
    length = log_ref.shape[0]
    row, col = grid_of(length, length)
    gap = log_ref[:, h : h + 1] - logt_ref[h : h + 1, :]
    return jnp.where(row >= col, jnp.exp(jnp.minimum(gap, 0.0)), 0.0)


def local_part(groups, v_ref, b_ref, c_ref, steps_ref, log_ref, logt_ref, y_ref, state_ref):
    heads = steps_ref.shape[1]
    per, size = heads // groups, v_ref.shape[1] // heads
    wide = per * size
    length = v_ref.shape[0]
    expand = spread(heads, size)
    to_end = jnp.exp(log_ref[length - 1 :, :] - log_ref[...])
    x = v_ref[...].astype(F32) * mm_exact(steps_ref[...], expand)
    xe = (x * mm_exact(to_end, expand)).astype(BF16)
    x = x.astype(BF16)
    for g in range(groups):
        keys = b_ref[:, g * NSTATE : (g + 1) * NSTATE]
        scores = mm(c_ref[:, g * NSTATE : (g + 1) * NSTATE], keys, NT)
        parts = []
        for r in range(per):
            h = g * per + r
            att = (scores * mixing_of(log_ref, logt_ref, h)).astype(BF16)
            parts.append(mm(att, x[:, h * size : (h + 1) * size]))
        y_ref[:, g * wide : (g + 1) * wide] = jnp.concatenate(parts, axis=1)
        state_ref[g * wide : (g + 1) * wide, :] = mm(
            xe[:, g * wide : (g + 1) * wide], keys, TN
        ).astype(BF16)


def enter_part(groups, y_ref, gate_ref, c_ref, log_ref, state_ref, out_ref, gated_ref):
    heads = log_ref.shape[1]
    per, size = heads // groups, y_ref.shape[1] // heads
    wide = per * size
    decay = mm_exact(jnp.exp(log_ref[...]), spread(heads, size))
    for g in range(groups):
        at = slice(g * wide, (g + 1) * wide)
        entered = mm(c_ref[:, g * NSTATE : (g + 1) * NSTATE], state_ref[at, :], NT) * decay[:, at]
        mixed = y_ref[:, at] + entered
        out_ref[:, at] = mixed
        gate = gate_ref[:, at].astype(F32)
        gated_ref[:, at] = (mixed * gate * jax.nn.sigmoid(gate)).astype(BF16)


def gate_part(groups, grad_ref, out_ref, gate_ref, c_ref, log_ref, gate_grad_ref, mixer_ref, state_ref):
    heads = log_ref.shape[1]
    wide = grad_ref.shape[1] // groups
    decay = mm_exact(jnp.exp(log_ref[...]), spread(heads, grad_ref.shape[1] // heads))
    for g in range(groups):
        at = slice(g * wide, (g + 1) * wide)
        gate = gate_ref[:, at].astype(F32)
        sig = jax.nn.sigmoid(gate)
        grad = grad_ref[:, at]
        gate_grad_ref[:, at] = (grad * out_ref[:, at] * sig * (1.0 + gate * (1.0 - sig))).astype(BF16)
        mixer = grad * gate * sig
        mixer_ref[:, at] = mixer
        keys = c_ref[:, g * NSTATE : (g + 1) * NSTATE]
        state_ref[at, :] = mm((mixer * decay[:, at]).astype(BF16), keys, TN).astype(BF16)


def inner_part(
    groups, v_ref, b_ref, c_ref, steps_ref, log_ref, logt_ref, mixer_ref, state_ref,
    out_keys_ref, in_part_ref, x_part_ref, base_ref,
):
    heads = steps_ref.shape[1]
    per, size = heads // groups, v_ref.shape[1] // heads
    wide = per * size
    length = v_ref.shape[0]
    row, col = grid_of(length, length)
    later = (row <= col).astype(BF16)
    expand = spread(heads, size)
    mixer = mixer_ref[...]
    decayed = mixer * mm_exact(jnp.exp(log_ref[...]), expand)
    decayed_low = decayed.astype(BF16)
    mixer = mixer.astype(BF16)
    x = (v_ref[...].astype(F32) * mm_exact(steps_ref[...], expand)).astype(BF16)
    entering = []
    _, head_at = grid_of(length, heads)
    pairs = jnp.zeros((length, heads), F32)
    for g in range(groups):
        at = slice(g * wide, (g + 1) * wide)
        keys_in = b_ref[:, g * NSTATE : (g + 1) * NSTATE]
        keys_out = c_ref[:, g * NSTATE : (g + 1) * NSTATE]
        scores = mm(keys_out, keys_in, NT)
        score_grad = jnp.zeros((length, length), F32)
        parts = []
        for r in range(per):
            h = g * per + r
            here = slice(h * size, (h + 1) * size)
            mixing = mixing_of(log_ref, logt_ref, h)
            att = scores * mixing
            att_grad = mm(mixer[:, here], x[:, here], NT)
            parts.append(mm(att.astype(BF16), mixer[:, here], TN))
            score_grad = score_grad + att_grad * mixing
            after = mm(later, (att_grad * att).astype(BF16))
            crossing = jnp.sum(jnp.where(col < row, after, 0.0), axis=1, keepdims=True)
            pairs = pairs + jnp.where(head_at == h, crossing, 0.0)
        x_part_ref[:, at] = jnp.concatenate(parts, axis=1)
        score_grad = score_grad.astype(BF16)
        state = state_ref[at, :]
        out_keys_ref[:, g * NSTATE : (g + 1) * NSTATE] = (
            mm(score_grad, keys_in) + mm(decayed_low[:, at], state)
        ).astype(BF16)
        in_part_ref[:, g * NSTATE : (g + 1) * NSTATE] = mm(score_grad, keys_out, TN)
        entering.append(decayed[:, at] * mm(keys_out, state, NT))
    entering = jnp.concatenate(entering, axis=1)
    sums = mm_exact(entering, fold(heads, size))
    base_ref[...] = pairs + mm_exact((row <= col).astype(F32), sums)


def outer_part(
    groups, after_ref, state_ref, v_ref, b_ref, steps_ref, log_ref, rates_ref,
    in_part_ref, x_part_ref, base_ref, values_ref, in_keys_ref, steps_grad_ref,
):
    heads = steps_ref.shape[1]
    per, size = heads // groups, v_ref.shape[1] // heads
    wide = per * size
    length = v_ref.shape[0]
    row, col = grid_of(length, length)
    expand = spread(heads, size)
    last = log_ref[length - 1 :, :]
    steps = mm_exact(steps_ref[...], expand)
    to_end = mm_exact(jnp.exp(last - log_ref[...]), expand)
    values = v_ref[...].astype(F32)
    xe = values * steps * to_end
    xe_low = xe.astype(BF16)
    leaving, direct = [], []
    _, head_at = grid_of(1, heads)
    passing = jnp.zeros((1, heads), F32)
    for g in range(groups):
        at = slice(g * wide, (g + 1) * wide)
        keys_in = b_ref[:, g * NSTATE : (g + 1) * NSTATE]
        for r in range(per):
            h = g * per + r
            here = slice(h * size, (h + 1) * size)
            both = after_ref[here, :] * state_ref[here, :].astype(F32)
            both = jnp.sum(jnp.sum(both, axis=0, keepdims=True), axis=1, keepdims=True)
            passing = passing + jnp.where(head_at == h, both, 0.0)
        after = after_ref[at, :].astype(BF16)
        reached = mm(keys_in, after, NT)
        x_grad = x_part_ref[:, at] + reached * to_end[:, at]
        values_ref[:, at] = (x_grad * steps[:, at]).astype(BF16)
        in_keys_ref[:, g * NSTATE : (g + 1) * NSTATE] = (
            in_part_ref[:, g * NSTATE : (g + 1) * NSTATE] + mm(xe_low[:, at], after)
        ).astype(BF16)
        leaving.append(reached * xe[:, at])
        direct.append(x_grad * values[:, at])
    gather = fold(heads, size)
    leaving = mm_exact(jnp.concatenate(leaving, axis=1), gather)
    direct = mm_exact(jnp.concatenate(direct, axis=1), gather)
    crossing = base_ref[...] + mm_exact((col < row).astype(F32), leaving) + jnp.exp(last) * passing
    steps_grad_ref[...] = direct - rates_ref[...] * crossing


class Sends:
    def __init__(self, sems):
        self.sems, self.used, self.open = sems, 0, []

    def copy(self, src, dst, landed, to):
        sem = self.sems.at[self.used]
        self.used += 1
        return pltpu.make_async_remote_copy(
            src_ref=src, dst_ref=dst, send_sem=sem, recv_sem=landed,
            device_id=to, device_id_type=MESH,
        )

    def send(self, cond, src, dst, landed, to):
        copy = self.copy(src, dst, landed, to)
        when(cond, copy.start)
        self.open.append((cond, copy))

    def finish(self):
        assert self.used <= self.sems.shape[0]
        for cond, copy in self.open:
            when(cond, copy.wait_send)


def when(cond, action):
    if cond is None:
        action()
    else:
        pl.when(cond)(action)


def both(a, b):
    return a if b is None else b if a is None else a & b


class Place:
    def __init__(self, n, m):
        self.n, self.m, self.chips = n, m, n // 2
        self.s, self.t = lax.axis_index("sp"), lax.axis_index("tp")
        self.z, self.c = self.s // 2, lax.rem(self.s, 2)
        self.mate = self.z * 2 + 1 - self.c

    def around(self):
        for d in range(1, self.chips):
            for sign in (1, -1):
                at = self.z + sign * d
                yield d, at, (at >= 0) & (at < self.chips)

    def planes(self):
        for d in range(1, self.m):
            yield lax.rem(self.t + d, self.m)


class Line:
    def __init__(self, place, sends, own, full, landed):
        self.p, self.sends, self.own, self.full, self.landed = place, sends, own, full, landed

    def put(self, cond, src, owner, to):
        self.sends.send(cond, src, self.full.at[owner], self.landed.at[owner], (to, self.p.t))

    def arrived(self, cond, owner):
        block = self.full.at[owner]
        copy = pltpu.make_async_remote_copy(
            src_ref=block, dst_ref=block, send_sem=self.landed.at[owner], recv_sem=self.landed.at[owner],
            device_id=(self.p.mate, self.p.t), device_id_type=MESH,
        )
        when(cond, copy.wait_recv)

    def begin(self, up=True, down=True):
        p = self.p
        if down:
            self.put(p.z > 0, self.own, p.s, p.s - 2)
            self.put(None, self.own, p.s, p.mate)
        if up:
            self.put(p.z < p.chips - 1, self.own, p.s, p.s + 2)

    def step(self, d):
        p = self.p
        below, above = p.s - 2 * d, p.s + 2 * d
        from_below, from_above = p.z >= d, p.z + d < p.chips
        self.arrived(from_below, below)
        if d < p.chips - 1:
            self.put(from_below & (p.z < p.chips - 1), self.full.at[below], below, p.s + 2)
        self.put(from_below, self.full.at[below], below, p.mate)
        self.arrived(from_above, above)
        if d < p.chips - 1:
            self.put(from_above & (p.z > 0), self.full.at[above], above, p.s - 2)
        self.put(from_above, self.full.at[above], above, p.mate)

    def end(self):
        for k in range(self.p.chips):
            self.arrived(None, 2 * k + 1 - self.p.c)


class Chain:
    def __init__(self, place, sends, first, own, mates, span, mate_span, carry, onward, landed, swapped):
        self.p, self.sends, self.first = place, sends, first
        self.own, self.mates, self.span, self.mate_span = own, mates, span, mate_span
        self.carry, self.onward, self.landed, self.swapped = carry, onward, landed, swapped
        self.starts = place.z == (0 if first == 0 else place.chips - 1)
        self.stops = place.z == (place.chips - 1 if first == 0 else 0)
        self.next = place.s + (2 if first == 0 else -2)

    def wait(self, cond, ref, sem):
        copy = pltpu.make_async_remote_copy(
            src_ref=ref, dst_ref=ref, send_sem=sem, recv_sem=sem,
            device_id=(self.p.mate, self.p.t), device_id_type=MESH,
        )
        when(cond, copy.wait_recv)

    def exchange(self):
        p = self.p
        self.sends.send(None, self.own, self.mates, self.swapped, (p.mate, p.t))

    def step(self, heads, size, only=None):
        p, c = self.p, self.p.c
        half = heads // 2
        rows = half * size

        def zero():
            self.carry[...] = jnp.zeros(self.carry.shape, self.carry.dtype)

        when(both(self.starts, only), zero)
        self.wait(both(~self.starts, only), self.carry.at[c], self.landed.at[0])
        self.sends.send(
            both(~self.starts, only), self.carry.at[c], self.carry.at[c], self.landed.at[1], (p.mate, p.t)
        )

        def advance():
            mine, other = jnp.exp(self.span[0:1, :]), jnp.exp(self.mate_span[0:1, :])
            near = c == self.first
            for r in range(half):
                at = pl.ds(pl.multiple_of(c * rows + r * size, size), size)
                low, high = slice(r, r + 1), slice(half + r, half + r + 1)
                w_mine = jnp.where(c == 0, mine[:, low], mine[:, high])
                w_other = jnp.where(c == 0, other[:, low], other[:, high])
                own, mate = self.own[at, :].astype(F32), self.mates[at, :].astype(F32)
                carried = self.carry[c, r * size : (r + 1) * size, :].astype(F32)
                a = jnp.where(near, w_mine, w_other) * carried + jnp.where(near, own, mate)
                b = jnp.where(near, w_other, w_mine) * a + jnp.where(near, mate, own)
                self.onward[r * size : (r + 1) * size, :] = b.astype(BF16)

        go = both(~self.stops, only)
        when(go, advance)
        self.sends.send(go, self.onward, self.carry.at[c], self.landed.at[0], (self.next, p.t))

    def finish(self, heads, size, target):
        p = self.p
        half = heads // 2
        rows = half * size
        self.wait(~self.starts, self.carry.at[1 - p.c], self.landed.at[1])
        other = jnp.exp(self.mate_span[0:1, :])
        near = p.c == self.first
        for h in range(heads):
            at = slice(h * size, (h + 1) * size)
            inside = slice((h % half) * size, (h % half + 1) * size)
            carried = self.carry[h // half, inside, :].astype(F32)
            through = other[:, h : h + 1] * carried + self.mates[at, :].astype(F32)
            target[at, :] = jnp.where(near, carried, through).astype(target.dtype)


def comm_kernel(
    cfg,
    v_ref, gate_ref, b_ref, c_ref, steps_ref, rates_ref, proj_ref, x_ref, g_ref, routes_ref, weights_ref,
    wg_hbm, wu_hbm, wd_hbm,
    dg_hbm, du_hbm, dd_hbm, grad_gate_ref, out_keys_ref, in_part_ref, x_part_ref, base_ref, log_ref,
    state_in, after_ref, all_stream, all_gated,
    wg, wu, wd, dw, logt_ref, y_ref, mixer_out, gated, own_state, mate_state, own_grad, mate_grad,
    span, mate_span, carry_f, onward_f, carry_b, onward_b, gated_grad, mixer_grad,
    picked_ref, parts, local, rows, act, gate_g, up_g, back, shares, reduced, returned, stream, full_proj,
    send_sems, load_sems, store_sems, dz_in, dp_in, rs_in, rt_in, st_in, as_in, proj_in, gated_in,
    fwd_in, bwd_in, swap_in,
):
    n, m, groups, capp, width, share = cfg
    p = Place(n, m)
    sends = Sends(send_sems)
    tokens, top = routes_ref.shape
    heads = steps_ref.shape[1]
    size = v_ref.shape[1] // heads
    slots = n * capp
    model = x_ref.shape[1]
    hidden = wg.shape[0]

    def wait(cond, ref, sem):
        copy = pltpu.make_async_remote_copy(
            src_ref=ref, dst_ref=ref, send_sem=sem, recv_sem=sem,
            device_id=(p.mate, p.t), device_id_type=MESH,
        )
        when(cond, copy.wait_recv)

    loads = [
        pltpu.make_async_copy(src, dst, load_sems.at[k])
        for k, (src, dst) in enumerate(((wg_hbm, wg), (wu_hbm, wu), (wd_hbm, wd)))
    ]
    for load in loads:
        load.start()
    barrier = pltpu.get_barrier_semaphore()
    for d in range(1, n):
        pl.semaphore_signal(barrier, inc=1, device_id=(lax.rem(p.s + d, n), p.t), device_id_type=MESH)
    for other in p.planes():
        pl.semaphore_signal(barrier, inc=1, device_id=(p.s, other), device_id_type=MESH)

    row, col = grid_of(tokens, tokens)
    drop = -steps_ref[...] * rates_ref[...]
    log = mm_exact((row >= col).astype(F32), drop)
    log_ref[...] = log
    logt_ref[...] = log.T
    span[...] = jnp.zeros(span.shape, F32)
    span[0:1, 0:heads] = log[tokens - 1 :, :]
    local_part(groups, v_ref, b_ref, c_ref, steps_ref, log_ref, logt_ref, y_ref, own_state)

    start = pl.multiple_of(p.t * width, 128)
    mine = pl.ds(start, width)
    _, expert = grid_of(tokens, n)
    _, slot = grid_of(tokens, slots)
    _, near = grid_of(tokens, 2 * capp)
    near = jnp.where(near < capp, p.s * capp + near, p.mate * capp + near - capp)
    hits = [expert == routes_ref[:, k : k + 1] for k in range(top)]
    named = sum(hit.astype(F32) for hit in hits)
    before = mm((row > col).astype(BF16), named.astype(BF16))
    every = jnp.zeros((tokens, slots), F32)
    every_near = jnp.zeros((tokens, 2 * capp), F32)
    grads = jnp.zeros((slots, width), F32)
    grads_near = jnp.zeros((2 * capp, model), F32)
    g_part = g_ref[:, mine].astype(F32)
    for k in range(top):
        rank = jnp.sum(jnp.where(hits[k], before, 0.0), axis=1, keepdims=True).astype(jnp.int32)
        at = routes_ref[:, k : k + 1] * capp + rank
        chosen = (slot == at).astype(F32)
        chosen_near = (near == at).astype(F32)
        every, every_near = every + chosen, every_near + chosen_near
        weight = weights_ref[:, k : k + 1]
        grads = grads + mm(chosen.astype(BF16), (g_part * weight).astype(BF16), TN)
        grads_near = grads_near + mm(
            chosen_near.astype(BF16), (g_ref[...].astype(F32) * weight).astype(BF16), TN
        )
    picked = every.astype(BF16)
    picked_ref[...] = picked
    parts[0] = mm(picked, x_ref[:, mine], TN).astype(BF16).reshape(n, capp, width)
    parts[1] = grads.astype(BF16).reshape(n, capp, width)
    x_near = mm(every_near.astype(BF16), x_ref[...], TN).astype(BF16)
    grads_near = grads_near.astype(BF16)
    local[0] = x_near[capp:]
    local[1] = grads_near[capp:]

    pl.semaphore_wait(barrier, n + m - 2)
    sends.send(None, local, rows.at[:, p.s], dz_in.at[p.s], (p.mate, p.t))
    forward = Chain(
        p, sends, 0, own_state, mate_state, span, mate_span, carry_f, onward_f, fwd_in, swap_in.at[0]
    )
    forward.exchange()
    sends.send(None, span, mate_span, swap_in.at[2], (p.mate, p.t))
    wait(None, mate_state, swap_in.at[0])
    wait(None, mate_span, swap_in.at[2])
    forward.step(heads, size, only=p.z == 0)
    for _, at, ok in p.around():
        for core in range(2):
            to = at * 2 + core
            sends.send(ok, parts.at[:, to], rows.at[:, p.s, :, mine], dz_in.at[p.s], (to, p.t))
    rows[0, p.s] = x_near[:capp]
    rows[1, p.s] = grads_near[:capp]
    line = Line(p, sends, proj_ref, full_proj, proj_in)
    line.begin(up=False)
    full_proj[p.s] = proj_ref[...]

    for d in range(1, p.chips):
        for sign in (1, -1):
            at = p.z + sign * d
            ok = (at >= 0) & (at < p.chips)
            for core in range(2):
                source = at * 2 + core
                wait(ok, rows.at[:, source, :, mine], dz_in.at[source])
            block = rows.at[:, pl.ds(2 * at, 2), :, mine]
            for other in p.planes():
                sends.send(ok, block, block, dp_in.at[at, p.t], (p.s, other))
        forward.step(heads, size, only=p.z == d)
    line.begin(down=False)
    forward.finish(heads, size, state_in)
    enter_part(groups, y_ref, gate_ref, c_ref, log_ref, state_in, mixer_out, gated)
    all_gated[p.s] = gated[...]
    line.step(1)
    wait(None, rows.at[:, p.mate], dz_in.at[p.mate])
    for _, at, ok in p.around():
        for other in p.planes():
            wait(ok, rows.at[:, pl.ds(2 * at, 2), :, pl.ds(pl.multiple_of(other * width, 128), width)], dp_in.at[at, other])

    for load in loads:
        load.wait()
    chunk = min(256, hidden)

    def experts(k, _):
        at = pl.ds(pl.multiple_of(k * chunk, chunk), chunk)
        in_rows = rows[0].reshape(slots, model)
        gate_pre = mm(in_rows, wg[at, :], NT)
        up_pre = mm(in_rows, wu[at, :], NT)
        act_grad = mm(rows[1].reshape(slots, model), wd[at, :], NT)
        gate_clamped = jnp.minimum(gate_pre, CLAMP_LIMIT)
        up_clamped = jnp.clip(up_pre, -CLAMP_LIMIT, CLAMP_LIMIT) + 1.0
        sig = jax.nn.sigmoid(SIGMOID_SCALE * gate_clamped)
        swish = gate_clamped * sig
        act[:, at] = (up_clamped * swish).astype(BF16)
        gate_g[:, at] = jnp.where(
            gate_pre < CLAMP_LIMIT,
            act_grad * up_clamped * sig * (1.0 + SIGMOID_SCALE * gate_clamped * (1.0 - sig)),
            0.0,
        ).astype(BF16)
        up_g[:, at] = jnp.where(jnp.abs(up_pre) < CLAMP_LIMIT, act_grad * swish, 0.0).astype(BF16)
        return 0

    lax.fori_loop(0, hidden // chunk, experts, 0)

    def backs(q, _):
        at = pl.ds(pl.multiple_of(q * width, 128), width)
        back[q] = (mm(gate_g[...], wg[:, at]) + mm(up_g[...], wu[:, at])).astype(BF16)
        return 0

    lax.fori_loop(0, m, backs, 0)
    pair = 2 * capp
    chunks = [lax.rem(p.z + d, p.chips) for d in range(1, p.chips + 1)]
    spans = [pl.ds(pl.multiple_of(at * pair, pair), pair) for at in chunks]
    for at, here in zip(chunks, spans):
        for other in p.planes():
            sends.send(None, back.at[other, here], shares.at[p.t, here], rs_in.at[at, p.t], (p.s, other))

    def weight_grads(k, _):
        at = pl.ds(pl.multiple_of(k * chunk, chunk), chunk)
        in_rows = rows[0].reshape(slots, model)
        dw[0, at, :] = mm(gate_g[:, at], in_rows, TN).astype(BF16)
        dw[1, at, :] = mm(up_g[:, at], in_rows, TN).astype(BF16)
        dw[2, at, :] = mm(act[:, at], rows[1].reshape(slots, model), TN).astype(BF16)
        return 0

    lax.fori_loop(0, hidden // chunk, weight_grads, 0)
    stores = [
        pltpu.make_async_copy(dw.at[k], dst, store_sems.at[k]) for k, dst in enumerate((dg_hbm, du_hbm, dd_hbm))
    ]
    for store in stores:
        store.start()
    if p.chips > 2:
        line.step(2)
    for k, (at, here) in enumerate(zip(chunks, spans)):
        total = back[p.t, here].astype(F32)
        for other in p.planes():
            wait(None, shares.at[other, here], rs_in.at[at, other])
            total = total + shares[other, here].astype(F32)
        reduced[pl.ds(2 * at, 2)] = total.astype(BF16).reshape(2, capp, width)
        if k < p.chips - 1:
            for core in range(2):
                to = 2 * at + core
                sends.send(None, reduced.at[to], returned.at[p.s], rt_in.at[p.s], (to, p.t))
        else:
            sends.send(None, reduced.at[p.mate], returned.at[p.s], rt_in.at[p.s], (p.mate, p.t))
            returned[p.s] = reduced[p.s]
    gather = Line(p, sends, gated, all_gated, gated_in)
    gather.begin()
    for d in range(3, p.chips):
        line.step(d)
    for d in range(1, n):
        source = lax.rem(p.s + d, n)
        wait(None, returned.at[source], rt_in.at[source])
    stream[:, mine] = (g_ref[:, mine].astype(F32) + mm(picked_ref[...], returned[...].reshape(slots, width))).astype(BF16)
    for other in p.planes():
        sends.send(None, stream.at[:, mine], stream.at[:, mine], st_in.at[p.t], (p.s, other))
    line.end()
    gather.step(1)
    for other in p.planes():
        wait(None, stream.at[:, pl.ds(pl.multiple_of(other * width, 128), width)], st_in.at[other])
    step = max(share, 128)

    def columns(j):
        return pl.ds(pl.multiple_of(j * share // step * step, 128), step)

    def to_all():
        for _, at, ok in p.around():
            for core in range(2):
                to = at * 2 + core
                sends.send(ok, stream.at[:, columns(to)], all_stream.at[p.s], as_in.at[p.s], (to, p.t))
        sends.send(None, stream.at[:, columns(p.mate)], all_stream.at[p.s], as_in.at[p.s], (p.mate, p.t))
        all_stream[p.s] = stream[:, columns(p.s)]

    to_all()
    gated_grad[...] = mm(stream[...], full_proj[...].reshape(model, v_ref.shape[1]))
    gate_part(groups, gated_grad, mixer_out, gate_ref, c_ref, log_ref, grad_gate_ref, mixer_grad, own_grad)
    backward = Chain(
        p, sends, 1, own_grad, mate_grad, span, mate_span, carry_b, onward_b, bwd_in, swap_in.at[1]
    )
    backward.exchange()
    wait(None, mate_grad, swap_in.at[1])
    backward.step(heads, size, only=p.z == p.chips - 1)
    inner_part(
        groups, v_ref, b_ref, c_ref, steps_ref, log_ref, logt_ref, mixer_grad, state_in,
        out_keys_ref, in_part_ref, x_part_ref, base_ref,
    )
    for d in range(1, p.chips):
        if d > 1:
            gather.step(d)
        backward.step(heads, size, only=p.z == p.chips - 1 - d)
    backward.finish(heads, size, after_ref)
    gather.end()
    for d in range(1, n):
        source = lax.rem(p.s + d, n)
        wait(None, all_stream.at[source], as_in.at[source])
    for store in stores:
        store.wait()
    sends.finish()


def last_kernel(
    cfg,
    dg_in, du_in, dd_in, grad_gate_in, out_keys_in, in_part_ref, x_part_ref, base_ref, log_ref,
    state_in, after_ref, all_stream, all_gated, v_ref, b_ref, steps_ref, rates_ref,
    dg_out, du_out, dd_out, proj_grad_ref, values_ref, grad_gate_ref, in_keys_ref, out_keys_ref, steps_grad_ref,
    passing, sums, sems,
):
    n, m, groups, capp, width, share = cfg
    ins = [pltpu.make_async_copy(src, passing.at[k], sems.at[k]) for k, src in enumerate((dg_in, du_in, dd_in))]
    outs = [pltpu.make_async_copy(passing.at[k], dst, sems.at[3 + k]) for k, dst in enumerate((dg_out, du_out, dd_out))]
    for copy in ins:
        copy.start()
    tokens = all_stream.shape[0] * all_stream.shape[1]
    step = all_stream.shape[2]
    grad = mm(all_stream[...].reshape(tokens, step), all_gated[...].reshape(tokens, all_gated.shape[2]), TN)
    if step == share:
        proj_grad_ref[...] = grad
    else:
        sums[...] = grad
        off = pl.multiple_of(lax.rem(lax.axis_index("sp"), step // share) * share, share)
        proj_grad_ref[...] = sums[pl.ds(off, share), :]
    for a, b in zip(ins, outs):
        a.wait()
        b.start()
    grad_gate_ref[...] = grad_gate_in[...]
    out_keys_ref[...] = out_keys_in[...]
    outer_part(
        groups, after_ref, state_in, v_ref, b_ref, steps_ref, log_ref, rates_ref,
        in_part_ref, x_part_ref, base_ref, values_ref, in_keys_ref, steps_grad_ref,
    )
    for copy in outs:
        copy.wait()


def body(
    mix_values, mix_gate, input_keys, output_keys, step_sizes, decay_rates, out_proj, expert_inputs,
    stream_grad, routes, route_weights, gate_proj, up_proj, down_proj,
):
    tokens, inner = mix_values.shape
    model = stream_grad.shape[1]
    top = routes.shape[1]
    n, m = lax.axis_size("sp"), lax.axis_size("tp")
    experts = gate_proj.shape[0] * n
    cap = 3 * tokens * top // (2 * experts)
    capp = -(-cap // 16) * 16
    slots = n * capp
    heads = step_sizes.shape[1]
    groups = input_keys.shape[1] // NSTATE
    width = model // m
    hidden = gate_proj.shape[1]
    share = model // n
    chips = n // 2
    step = max(share, 128)
    rates = decay_rates.reshape(1, heads)
    cfg = (n, m, groups, capp, width, share)
    vm, anyw = pl.BlockSpec(memory_space=pltpu.VMEM), pl.BlockSpec(memory_space=pl.ANY)
    keys_shape = input_keys.shape
    weight = (hidden, model)
    dma = pltpu.SemaphoreType.DMA
    sent = (
        3 + 1 + 4 * (chips - 1) + 2 * (chips - 1) * (m - 1) + 2 * (3 + 4 * (chips - 1))
        + chips * (m - 1) + 2 * chips + (m - 1) + 4 * chips + 2 * 2 * (chips + 1) + 8
    )
    mids = pl.pallas_call(
        functools.partial(comm_kernel, cfg),
        out_shape=[
            out(weight, BF16), out(weight, BF16), out(weight, BF16),
            out((tokens, inner), BF16), out(keys_shape, BF16), out(keys_shape, F32),
            out((tokens, inner), F32), out((tokens, heads), F32), out((tokens, heads), F32),
            out((inner, NSTATE), BF16), out((inner, NSTATE), F32),
            out((n, tokens, step), BF16), out((n, tokens, inner), BF16),
        ],
        in_specs=[vm] * 11 + [anyw] * 3,
        out_specs=[anyw] * 3 + [vm] * 10,
        scratch_shapes=[
            pltpu.VMEM(weight, BF16), pltpu.VMEM(weight, BF16), pltpu.VMEM(weight, BF16),
            pltpu.VMEM((3,) + weight, BF16),
            pltpu.VMEM((heads, tokens), F32),
            pltpu.VMEM((tokens, inner), F32), pltpu.VMEM((tokens, inner), F32), pltpu.VMEM((tokens, inner), BF16),
            pltpu.VMEM((inner, NSTATE), BF16), pltpu.VMEM((inner, NSTATE), BF16),
            pltpu.VMEM((inner, NSTATE), BF16), pltpu.VMEM((inner, NSTATE), BF16),
            pltpu.VMEM((8, 128), F32), pltpu.VMEM((8, 128), F32),
            pltpu.VMEM((2, inner // 2, NSTATE), BF16), pltpu.VMEM((inner // 2, NSTATE), BF16),
            pltpu.VMEM((2, inner // 2, NSTATE), BF16), pltpu.VMEM((inner // 2, NSTATE), BF16),
            pltpu.VMEM((tokens, inner), F32), pltpu.VMEM((tokens, inner), F32),
            pltpu.VMEM((tokens, slots), BF16),
            pltpu.VMEM((2, n, capp, width), BF16),
            pltpu.VMEM((2, capp, model), BF16),
            pltpu.VMEM((2, n, capp, model), BF16),
            pltpu.VMEM((slots, hidden), BF16), pltpu.VMEM((slots, hidden), BF16), pltpu.VMEM((slots, hidden), BF16),
            pltpu.VMEM((m, slots, width), BF16), pltpu.VMEM((m, slots, width), BF16),
            pltpu.VMEM((n, capp, width), BF16), pltpu.VMEM((n, capp, width), BF16),
            pltpu.VMEM((tokens, model), BF16),
            pltpu.VMEM((n,) + out_proj.shape, BF16),
            dma((sent,)), dma((3,)), dma((3,)),
            dma((n,)), dma((chips, m)), dma((chips, m)), dma((n,)), dma((m,)), dma((n,)), dma((n,)), dma((n,)),
            dma((2,)), dma((2,)), dma((3,)),
        ],
        cost_estimate=pl.CostEstimate(flops=10**10, bytes_accessed=3 * 10**7, transcendentals=0),
        compiler_params=pltpu.CompilerParams(
            collective_id=0, has_side_effects=True, vmem_limit_bytes=60 * 2**20
        ),
    )(
        mix_values, mix_gate, input_keys, output_keys, step_sizes, rates, out_proj, expert_inputs,
        stream_grad, routes, route_weights,
        gate_proj.reshape(weight), up_proj.reshape(weight), down_proj.reshape(weight),
    )
    log = mids[8]
    outs = pl.pallas_call(
        functools.partial(last_kernel, cfg),
        out_shape=[
            out(weight, BF16), out(weight, BF16), out(weight, BF16),
            out((share, inner), F32), out((tokens, inner), BF16), out((tokens, inner), BF16),
            out(keys_shape, BF16), out(keys_shape, BF16), out((tokens, heads), F32),
        ],
        in_specs=[anyw] * 3 + [vm] * 14,
        out_specs=[anyw] * 3 + [vm] * 6,
        scratch_shapes=[pltpu.VMEM((3,) + weight, BF16), pltpu.VMEM((step, inner), F32), dma((6,))],
        cost_estimate=pl.CostEstimate(flops=10**9, bytes_accessed=2 * 10**7, transcendentals=0),
        compiler_params=pltpu.CompilerParams(vmem_limit_bytes=40 * 2**20),
    )(*mids, mix_values, input_keys, step_sizes, rates)
    shape = gate_proj.shape
    return tuple(o.reshape(shape) for o in outs[:3]) + tuple(outs[3:])


def solution(mesh):
    return jax.shard_map(
        body,
        mesh=mesh,
        in_specs=(
            P("sp", "tp"), P("sp", "tp"), P("sp", "tp"), P("sp", "tp"), P("sp", "tp"), P("tp"),
            P("sp", "tp"), P("sp", None), P("sp", None), P("sp", None), P("sp", None),
            P("sp", "tp", None), P("sp", "tp", None), P("sp", "tp", None),
        ),
        out_specs=(
            P("sp", "tp", None), P("sp", "tp", None), P("sp", "tp", None),
            P("sp", "tp"), P("sp", "tp"), P("sp", "tp"), P("sp", "tp"), P("sp", "tp"), P("sp", "tp"),
        ),
        check_vma=False,
    )
```

```python
import functools

import jax
import jax.numpy as jnp
from jax import lax
from jax.experimental import pallas as pl
from jax.experimental.pallas import tpu as pltpu
from jax.sharding import PartitionSpec as P

NSTATE = 128
CLAMP_LIMIT = 7.0
SIGMOID_SCALE = 1.702
HIGHEST = lax.Precision.HIGHEST
F32 = jnp.float32
BF16 = jnp.bfloat16
NN = (((1,), (0,)), ((), ()))
NT = (((1,), (1,)), ((), ()))
TN = (((0,), (0,)), ((), ()))
MESH = pl.DeviceIdType.MESH


def mm(a, b, dims=NN):
    return lax.dot_general(a, b, dims, preferred_element_type=F32)


def mm_exact(a, b, dims=NN):
    return lax.dot_general(a, b, dims, precision=HIGHEST, preferred_element_type=F32)


def grid_of(rows, cols):
    return (
        lax.broadcasted_iota(jnp.int32, (rows, cols), 0),
        lax.broadcasted_iota(jnp.int32, (rows, cols), 1),
    )


def spread(heads, size):
    at, col = grid_of(heads, heads * size)
    return ((col >= at * size) & (col < (at + 1) * size)).astype(F32)


def fold(heads, size):
    col, at = grid_of(heads * size, heads)
    return ((col >= at * size) & (col < (at + 1) * size)).astype(F32)


def out(shape, dtype):
    return jax.ShapeDtypeStruct(shape, dtype)


def mixing_of(log_ref, logt_ref, h):
    length = log_ref.shape[0]
    row, col = grid_of(length, length)
    gap = log_ref[:, h : h + 1] - logt_ref[h : h + 1, :]
    return jnp.where(row >= col, jnp.exp(jnp.minimum(gap, 0.0)), 0.0)


def local_part(groups, v_ref, b_ref, c_ref, steps_ref, log_ref, logt_ref, y_ref, state_ref):
    heads = steps_ref.shape[1]
    per, size = heads // groups, v_ref.shape[1] // heads
    wide = per * size
    length = v_ref.shape[0]
    expand = spread(heads, size)
    to_end = jnp.exp(log_ref[length - 1 :, :] - log_ref[...])
    x = v_ref[...].astype(F32) * mm_exact(steps_ref[...], expand)
    xe = (x * mm_exact(to_end, expand)).astype(BF16)
    x = x.astype(BF16)
    for g in range(groups):
        keys = b_ref[:, g * NSTATE : (g + 1) * NSTATE]
        scores = mm(c_ref[:, g * NSTATE : (g + 1) * NSTATE], keys, NT)
        parts = []
        for r in range(per):
            h = g * per + r
            att = (scores * mixing_of(log_ref, logt_ref, h)).astype(BF16)
            parts.append(mm(att, x[:, h * size : (h + 1) * size]))
        y_ref[:, g * wide : (g + 1) * wide] = jnp.concatenate(parts, axis=1)
        state_ref[g * wide : (g + 1) * wide, :] = mm(
            xe[:, g * wide : (g + 1) * wide], keys, TN
        ).astype(BF16)


def enter_part(groups, y_ref, gate_ref, c_ref, log_ref, state_ref, out_ref, gated_ref):
    heads = log_ref.shape[1]
    per, size = heads // groups, y_ref.shape[1] // heads
    wide = per * size
    decay = mm_exact(jnp.exp(log_ref[...]), spread(heads, size))
    for g in range(groups):
        at = slice(g * wide, (g + 1) * wide)
        entered = mm(c_ref[:, g * NSTATE : (g + 1) * NSTATE], state_ref[at, :], NT) * decay[:, at]
        mixed = y_ref[:, at] + entered
        out_ref[:, at] = mixed
        gate = gate_ref[:, at].astype(F32)
        gated_ref[:, at] = (mixed * gate * jax.nn.sigmoid(gate)).astype(BF16)


def gate_part(groups, grad_ref, out_ref, gate_ref, c_ref, log_ref, gate_grad_ref, mixer_ref, state_ref):
    heads = log_ref.shape[1]
    wide = grad_ref.shape[1] // groups
    decay = mm_exact(jnp.exp(log_ref[...]), spread(heads, grad_ref.shape[1] // heads))
    for g in range(groups):
        at = slice(g * wide, (g + 1) * wide)
        gate = gate_ref[:, at].astype(F32)
        sig = jax.nn.sigmoid(gate)
        grad = grad_ref[:, at]
        gate_grad_ref[:, at] = (grad * out_ref[:, at] * sig * (1.0 + gate * (1.0 - sig))).astype(BF16)
        mixer = grad * gate * sig
        mixer_ref[:, at] = mixer
        keys = c_ref[:, g * NSTATE : (g + 1) * NSTATE]
        state_ref[at, :] = mm((mixer * decay[:, at]).astype(BF16), keys, TN).astype(BF16)


def inner_part(
    groups, v_ref, b_ref, c_ref, steps_ref, log_ref, logt_ref, mixer_ref, state_ref,
    out_keys_ref, in_part_ref, x_part_ref, base_ref,
):
    heads = steps_ref.shape[1]
    per, size = heads // groups, v_ref.shape[1] // heads
    wide = per * size
    length = v_ref.shape[0]
    row, col = grid_of(length, length)
    later = (row <= col).astype(BF16)
    expand = spread(heads, size)
    mixer = mixer_ref[...]
    decayed = mixer * mm_exact(jnp.exp(log_ref[...]), expand)
    decayed_low = decayed.astype(BF16)
    mixer = mixer.astype(BF16)
    x = (v_ref[...].astype(F32) * mm_exact(steps_ref[...], expand)).astype(BF16)
    entering = []
    _, head_at = grid_of(length, heads)
    pairs = jnp.zeros((length, heads), F32)
    for g in range(groups):
        at = slice(g * wide, (g + 1) * wide)
        keys_in = b_ref[:, g * NSTATE : (g + 1) * NSTATE]
        keys_out = c_ref[:, g * NSTATE : (g + 1) * NSTATE]
        scores = mm(keys_out, keys_in, NT)
        score_grad = jnp.zeros((length, length), F32)
        parts = []
        for r in range(per):
            h = g * per + r
            here = slice(h * size, (h + 1) * size)
            mixing = mixing_of(log_ref, logt_ref, h)
            att = scores * mixing
            att_grad = mm(mixer[:, here], x[:, here], NT)
            parts.append(mm(att.astype(BF16), mixer[:, here], TN))
            score_grad = score_grad + att_grad * mixing
            after = mm(later, (att_grad * att).astype(BF16))
            crossing = jnp.sum(jnp.where(col < row, after, 0.0), axis=1, keepdims=True)
            pairs = pairs + jnp.where(head_at == h, crossing, 0.0)
        x_part_ref[:, at] = jnp.concatenate(parts, axis=1)
        score_grad = score_grad.astype(BF16)
        state = state_ref[at, :]
        out_keys_ref[:, g * NSTATE : (g + 1) * NSTATE] = (
            mm(score_grad, keys_in) + mm(decayed_low[:, at], state)
        ).astype(BF16)
        in_part_ref[:, g * NSTATE : (g + 1) * NSTATE] = mm(score_grad, keys_out, TN)
        entering.append(decayed[:, at] * mm(keys_out, state, NT))
    entering = jnp.concatenate(entering, axis=1)
    sums = mm_exact(entering, fold(heads, size))
    base_ref[...] = pairs + mm_exact((row <= col).astype(F32), sums)


def outer_part(
    groups, after_ref, state_ref, v_ref, b_ref, steps_ref, log_ref, rates_ref,
    in_part_ref, x_part_ref, base_ref, values_ref, in_keys_ref, steps_grad_ref,
):
    heads = steps_ref.shape[1]
    per, size = heads // groups, v_ref.shape[1] // heads
    wide = per * size
    length = v_ref.shape[0]
    row, col = grid_of(length, length)
    expand = spread(heads, size)
    last = log_ref[length - 1 :, :]
    steps = mm_exact(steps_ref[...], expand)
    to_end = mm_exact(jnp.exp(last - log_ref[...]), expand)
    values = v_ref[...].astype(F32)
    xe = values * steps * to_end
    xe_low = xe.astype(BF16)
    leaving, direct = [], []
    _, head_at = grid_of(1, heads)
    passing = jnp.zeros((1, heads), F32)
    for g in range(groups):
        at = slice(g * wide, (g + 1) * wide)
        keys_in = b_ref[:, g * NSTATE : (g + 1) * NSTATE]
        for r in range(per):
            h = g * per + r
            here = slice(h * size, (h + 1) * size)
            both = after_ref[here, :] * state_ref[here, :].astype(F32)
            both = jnp.sum(jnp.sum(both, axis=0, keepdims=True), axis=1, keepdims=True)
            passing = passing + jnp.where(head_at == h, both, 0.0)
        after = after_ref[at, :].astype(BF16)
        reached = mm(keys_in, after, NT)
        x_grad = x_part_ref[:, at] + reached * to_end[:, at]
        values_ref[:, at] = (x_grad * steps[:, at]).astype(BF16)
        in_keys_ref[:, g * NSTATE : (g + 1) * NSTATE] = (
            in_part_ref[:, g * NSTATE : (g + 1) * NSTATE] + mm(xe_low[:, at], after)
        ).astype(BF16)
        leaving.append(reached * xe[:, at])
        direct.append(x_grad * values[:, at])
    gather = fold(heads, size)
    leaving = mm_exact(jnp.concatenate(leaving, axis=1), gather)
    direct = mm_exact(jnp.concatenate(direct, axis=1), gather)
    crossing = base_ref[...] + mm_exact((col < row).astype(F32), leaving) + jnp.exp(last) * passing
    steps_grad_ref[...] = (direct - rates_ref[...] * crossing).T


class Phase:
    def __init__(self):
        self.scope = None

    def __call__(self, name):
        if self.scope is not None:
            self.scope.__exit__(None, None, None)
        self.scope = name and jax.named_scope(name)
        if self.scope is not None:
            self.scope.__enter__()


class Sends:
    def __init__(self, sems):
        self.sems, self.used, self.open = sems, 0, []

    def block(self, count):
        self.used += count
        return self.used - count

    def copy(self, src, dst, landed, to, at):
        sem = self.sems.at[self.block(1) if at is None else at]
        return pltpu.make_async_remote_copy(
            src_ref=src, dst_ref=dst, send_sem=sem, recv_sem=landed,
            device_id=to, device_id_type=MESH,
        )

    def send(self, cond, src, dst, landed, to, at=None):
        copy = self.copy(src, dst, landed, to, at)
        when(cond, copy.start)
        self.open.append((cond, copy))

    def finish(self):
        assert self.used <= self.sems.shape[0]
        for cond, copy in self.open:
            when(cond, copy.wait_send)


def when(cond, action):
    if cond is None:
        action()
    else:
        pl.when(cond)(action)


def both(a, b):
    return a if b is None else b if a is None else a & b


class Place:
    def __init__(self, n, m):
        self.n, self.m, self.chips = n, m, n // 2
        self.s, self.t = lax.axis_index("sp"), lax.axis_index("tp")
        self.z, self.c = self.s // 2, lax.rem(self.s, 2)
        self.mate = self.z * 2 + 1 - self.c

    def around(self):
        for d in range(1, self.chips):
            for sign in (1, -1):
                at = self.z + sign * d
                yield d, at, (at >= 0) & (at < self.chips)

    def wait(self, cond, ref, sem):
        copy = pltpu.make_async_remote_copy(
            src_ref=ref, dst_ref=ref, send_sem=sem, recv_sem=sem,
            device_id=(self.mate, self.t), device_id_type=MESH,
        )
        when(cond, copy.wait_recv)

    def planes(self):
        for d in range(1, self.m):
            yield lax.rem(self.t + d, self.m)


class Line:
    def __init__(self, place, sends, own, block, landed):
        self.p, self.sends, self.own, self.block, self.landed = place, sends, own, block, landed

    def put(self, cond, src, owner, to):
        self.sends.send(cond, src, self.block(owner), self.landed.at[owner], (to, self.p.t))

    def begin(self, middle=None):
        p = self.p
        down, up = p.z > 0, p.z < p.chips - 1
        down_middle, up_middle = p.z == p.chips // 2, p.z == p.chips // 2 - 1
        if middle is None:
            self.put(down, self.own, p.s, p.s - 2)
            self.put(up, self.own, p.s, p.s + 2)
        elif middle:
            self.put(down_middle, self.own, p.s, p.s - 2)
            self.put(up_middle, self.own, p.s, p.s + 2)
        else:
            self.put(down & ~down_middle, self.own, p.s, p.s - 2)
            self.put(up & ~up_middle, self.own, p.s, p.s + 2)
        if not middle:
            self.put(None, self.own, p.s, p.mate)

    def step(self, d):
        p = self.p
        below, above = p.s - 2 * d, p.s + 2 * d
        from_below, from_above = p.z >= d, p.z + d < p.chips
        p.wait(from_below, self.block(below), self.landed.at[below])
        if d < p.chips - 1:
            self.put(from_below & (p.z < p.chips - 1), self.block(below), below, p.s + 2)
        self.put(from_below, self.block(below), below, p.mate)
        p.wait(from_above, self.block(above), self.landed.at[above])
        if d < p.chips - 1:
            self.put(from_above & (p.z > 0), self.block(above), above, p.s - 2)
        self.put(from_above, self.block(above), above, p.mate)

    def end(self):
        for k in range(self.p.chips):
            owner = 2 * k + 1 - self.p.c
            self.p.wait(None, self.block(owner), self.landed.at[owner])


class Chain:
    def __init__(self, place, sends, first, own, mates, span, mate_span, carry, onward, landed, swapped):
        self.p, self.sends, self.first = place, sends, first
        self.own, self.mates, self.span, self.mate_span = own, mates, span, mate_span
        self.carry, self.onward, self.landed, self.swapped = carry, onward, landed, swapped
        self.starts = place.z == (0 if first == 0 else place.chips - 1)
        self.stops = place.z == (place.chips - 1 if first == 0 else 0)
        self.next = place.s + (2 if first == 0 else -2)
        self.at = sends.block(2)

    def exchange(self):
        p = self.p
        self.sends.send(None, self.own, self.mates, self.swapped, (p.mate, p.t))

    def step(self, heads, size, only=None):
        p, c = self.p, self.p.c
        half = heads // 2
        rows = half * size

        def zero():
            self.carry[...] = jnp.zeros(self.carry.shape, self.carry.dtype)

        when(both(self.starts, only), zero)
        self.p.wait(both(~self.starts, only), self.carry.at[c], self.landed.at[0])
        self.sends.send(
            both(~self.starts, only), self.carry.at[c], self.carry.at[c], self.landed.at[1], (p.mate, p.t), self.at
        )

        def advance():
            mine, other = jnp.exp(self.span[0:1, :]), jnp.exp(self.mate_span[0:1, :])
            near = c == self.first
            for r in range(half):
                at = pl.ds(pl.multiple_of(c * rows + r * size, size), size)
                low, high = slice(r, r + 1), slice(half + r, half + r + 1)
                w_mine = jnp.where(c == 0, mine[:, low], mine[:, high])
                w_other = jnp.where(c == 0, other[:, low], other[:, high])
                own, mate = self.own[at, :].astype(F32), self.mates[at, :].astype(F32)
                carried = self.carry[c, r * size : (r + 1) * size, :].astype(F32)
                a = jnp.where(near, w_mine, w_other) * carried + jnp.where(near, own, mate)
                b = jnp.where(near, w_other, w_mine) * a + jnp.where(near, mate, own)
                self.onward[r * size : (r + 1) * size, :] = b.astype(BF16)

        go = both(~self.stops, only)
        when(go, advance)
        self.sends.send(go, self.onward, self.carry.at[c], self.landed.at[0], (self.next, p.t), self.at + 1)

    def finish(self, heads, size, target):
        p = self.p
        half = heads // 2
        rows = half * size
        self.p.wait(~self.starts, self.carry.at[1 - p.c], self.landed.at[1])
        other = jnp.exp(self.mate_span[0:1, :])
        near = p.c == self.first
        for h in range(heads):
            at = slice(h * size, (h + 1) * size)
            inside = slice((h % half) * size, (h % half + 1) * size)
            carried = self.carry[h // half, inside, :].astype(F32)
            through = other[:, h : h + 1] * carried + self.mates[at, :].astype(F32)
            target[at, :] = jnp.where(near, carried, through).astype(target.dtype)


def first_kernel(out_ref):
    out_ref[...] = jnp.zeros(out_ref.shape, out_ref.dtype)


def comm_kernel(
    cfg,
    v_ref, gate_ref, b_ref, c_ref, steps_t_ref, rates_ref, proj_ref, x_ref, g_ref, routes_t_ref, weights_t_ref,
    first_ref, wg_hbm, wu_hbm, wd_hbm,
    dg_ref, du_ref, dd_ref, grad_gate_ref, out_keys_ref, in_part_ref, x_part_ref, base_ref, log_ref,
    state_in, after_ref, all_stream, all_gated, steps_ref,
    wg, wu, wd, logt_ref, y_ref, mixer_out, gated, own_state, mate_state, own_grad, mate_grad,
    span, mate_span, carry_f, onward_f, carry_b, onward_b, gated_grad, mixer_grad,
    picked_ref, parts, local, rows, act, gate_g, up_g, back, shares, hop, reduced, returned, stream, full_proj,
    send_sems, load_sems, dz_in, dp_in, dq_in, hop_in, rs_in, rt_in, st_in, as_in, ag_in,
    low_in, high_in, gated_in, fwd_in, bwd_in, swap_in,
):
    n, m, groups, capp, width, share = cfg
    p = Place(n, m)
    wait = p.wait
    sends = Sends(send_sems)
    phase = Phase()
    top, tokens = routes_t_ref.shape
    heads = steps_t_ref.shape[0]
    size = v_ref.shape[1] // heads
    slots = n * capp
    model = x_ref.shape[1]
    hidden = wg.shape[0]
    quad = m == 4
    by_x, by_y, across = p.t + 1 - 2 * lax.rem(p.t, 2), lax.rem(p.t + 2, 4), 3 - p.t

    def cols(t):
        return pl.ds(pl.multiple_of(t * width, 128), width)

    mine = cols(p.t)

    phase("barrier")
    pairs = ((wg_hbm, wg), (wu_hbm, wu), (wd_hbm, wd))
    loads = [pltpu.make_async_copy(src, dst, load_sems.at[k]) for k, (src, dst) in enumerate(pairs)]
    for load in loads:
        load.start()
    barrier = pltpu.get_barrier_semaphore()
    for d in range(1, n):
        pl.semaphore_signal(barrier, inc=1, device_id=(lax.rem(p.s + d, n), p.t), device_id_type=MESH)
    for other in p.planes():
        pl.semaphore_signal(barrier, inc=1, device_id=(p.s, other), device_id_type=MESH)
    half_rows = proj_ref.shape[0] // 2
    low, high = pl.ds(0, half_rows), pl.ds(half_rows, half_rows)
    line_a = Line(p, sends, proj_ref.at[low], lambda s: full_proj.at[s, low], low_in)
    line_b = Line(p, sends, proj_ref.at[high], lambda s: full_proj.at[s, high], high_in)

    phase("slots")
    routes = routes_t_ref[...].T
    weights = weights_t_ref[...].T
    row, col = grid_of(tokens, tokens)
    _, expert = grid_of(tokens, n)
    _, slot = grid_of(tokens, slots)
    _, near = grid_of(tokens, 2 * capp)
    near = jnp.where(near < capp, p.s * capp + near, p.mate * capp + near - capp)
    hits = [expert == routes[:, k : k + 1] for k in range(top)]
    named = sum(hit.astype(F32) for hit in hits)
    before = mm((row > col).astype(BF16), named.astype(BF16))
    every = jnp.zeros((tokens, slots), F32)
    every_near = jnp.zeros((tokens, 2 * capp), F32)
    grads = jnp.zeros((slots, width), F32)
    g_part = g_ref[:, mine].astype(F32)
    nears = []
    for k in range(top):
        rank = jnp.sum(jnp.where(hits[k], before, 0.0), axis=1, keepdims=True).astype(jnp.int32)
        at = routes[:, k : k + 1] * capp + rank
        chosen = (slot == at).astype(F32)
        chosen_near = (near == at).astype(F32)
        every, every_near = every + chosen, every_near + chosen_near
        weight = weights[:, k : k + 1]
        grads = grads + mm(chosen.astype(BF16), (g_part * weight).astype(BF16), TN)
        nears.append((chosen_near.astype(BF16), weight))
    picked = every.astype(BF16)
    parts[0] = mm(picked, x_ref[:, mine], TN).astype(BF16).reshape(n, capp, width)
    parts[1] = grads.astype(BF16).reshape(n, capp, width)
    phase("dispatch")
    pl.semaphore_wait(barrier, n + m - 2)
    base = sends.block(n)
    for _, at, ok in p.around():
        for core in range(2):
            to = at * 2 + core
            sends.send(ok, parts.at[:, to], rows.at[:, p.s, :, mine], dz_in.at[p.s], (to, p.t), base + to)
    phase("near")
    picked_ref[...] = picked
    x_near = mm(every_near.astype(BF16), x_ref[...], TN).astype(BF16)
    grads_near = sum(
        mm(chosen, (g_ref[...].astype(F32) * weight).astype(BF16), TN) for chosen, weight in nears
    ).astype(BF16)
    local[0] = x_near[capp:]
    local[1] = grads_near[capp:]
    sends.send(None, local, rows.at[:, p.s], dz_in.at[p.s], (p.mate, p.t))
    rows[0, p.s] = x_near[:capp]
    rows[1, p.s] = grads_near[:capp]

    phase("local")
    steps_ref[...] = steps_t_ref[...].T
    log = mm_exact((row >= col).astype(F32), -steps_ref[...] * rates_ref[...])
    log_ref[...] = log
    logt_ref[...] = log.T
    span[...] = jnp.zeros(span.shape, F32)
    span[0:1, 0:heads] = log[tokens - 1 :, :]
    local_part(groups, v_ref, b_ref, c_ref, steps_ref, log_ref, logt_ref, y_ref, own_state)
    forward = Chain(
        p, sends, 0, own_state, mate_state, span, mate_span, carry_f, onward_f, fwd_in, swap_in.at[0]
    )
    forward.exchange()
    sends.send(None, span, mate_span, swap_in.at[2], (p.mate, p.t))

    def pair_of(at, t):
        return rows.at[:, pl.ds(2 * at, 2), :, cols(t)]

    relay_base, turn_base = sends.block(p.chips * m), sends.block(p.chips * 2)

    def relay(d, only=None):
        phase(f"relay{d}")
        for sign in (1, -1):
            at = p.z + sign * d
            ok = both((at >= 0) & (at < p.chips), only)
            for core in range(2):
                source = at * 2 + core
                wait(ok, rows.at[:, source, :, mine], dz_in.at[source])
            block = pair_of(at, p.t)
            for other in (by_x, by_y) if quad else p.planes():
                sends.send(ok, block, block, dp_in.at[at, p.t], (p.s, other), relay_base + at * m + other)

    def turn(d):
        if not quad:
            return
        phase(f"turn{d}")
        for sign in (1, -1):
            at = p.z + sign * d
            ok = (at >= 0) & (at < p.chips)
            for k, (source, to) in enumerate(((by_x, by_y), (by_y, by_x))):
                wait(ok, pair_of(at, source), dp_in.at[at, source])
                block = rows.at[k, pl.ds(2 * at, 2), :, cols(source)]
                sends.send(ok, block, block, dq_in.at[at, k], (p.s, to), turn_base + at * 2 + k)

    side = p.chips // 2

    def landed(ok, at):
        ok = ok & (at != p.z)
        if quad:
            for k in range(2):
                wait(ok, rows.at[k, pl.ds(2 * at, 2), :, cols(across)], dq_in.at[at, k])
        else:
            for other in p.planes():
                wait(ok, pair_of(at, other), dp_in.at[at, other])

    chunk = min(256, hidden)
    half = slots // 2
    flip = p.z // side
    sides = (flip, 1 - flip)
    pair = 2 * capp

    def in_side(side_at):
        return [(side_at * side + k) for k in range(side)]

    def experts_of(side_at):
        sources = pl.ds(side_at * (n // 2), n // 2)
        here = pl.ds(pl.multiple_of(side_at * half, half), half)

        def experts(k, _):
            at = pl.ds(pl.multiple_of(k * chunk, chunk), chunk)
            in_rows = rows[0, sources].reshape(half, model)
            gate_pre = mm(in_rows, wg[at, :], NT)
            up_pre = mm(in_rows, wu[at, :], NT)
            act_grad = mm(rows[1, sources].reshape(half, model), wd[at, :], NT)
            gate_clamped = jnp.minimum(gate_pre, CLAMP_LIMIT)
            up_clamped = jnp.clip(up_pre, -CLAMP_LIMIT, CLAMP_LIMIT) + 1.0
            sig = jax.nn.sigmoid(SIGMOID_SCALE * gate_clamped)
            swish = gate_clamped * sig
            act[here, at] = (up_clamped * swish).astype(BF16)
            gate_g[here, at] = jnp.where(
                gate_pre < CLAMP_LIMIT,
                act_grad * up_clamped * sig * (1.0 + SIGMOID_SCALE * gate_clamped * (1.0 - sig)),
                0.0,
            ).astype(BF16)
            up_g[here, at] = jnp.where(jnp.abs(up_pre) < CLAMP_LIMIT, act_grad * swish, 0.0).astype(BF16)
            return 0

        lax.fori_loop(0, hidden // chunk, experts, 0)

        def backs(q, _):
            at = cols(q)
            back[q, here] = (mm(gate_g[here, :], wg[:, at]) + mm(up_g[here, :], wu[:, at])).astype(BF16)
            return 0

        lax.fori_loop(0, m, backs, 0)

    def span_of(at):
        return pl.ds(pl.multiple_of(at * pair, pair), pair)

    def halves_of(at):
        return [pl.ds(pl.multiple_of(at * pair + k * capp, capp), capp) for k in range(2)]

    def reduce_send(at):
        if quad:
            first, second = halves_of(at)
            sends.send(None, back.at[across, first], hop.at[at, 0], hop_in.at[at, 0], (p.s, by_x))
            sends.send(None, back.at[across, second], hop.at[at, 1], hop_in.at[at, 1], (p.s, by_y))
        else:
            here = span_of(at)
            for other in p.planes():
                sends.send(None, back.at[other, here], shares.at[p.t, here], rs_in.at[at, p.t], (p.s, other))

    def reduce_turn(at):
        if not quad:
            return
        here = span_of(at)
        for k, (to, part) in enumerate(zip((by_y, by_x), halves_of(at))):
            wait(None, hop.at[at, k], hop_in.at[at, k])
            back[to, part] = (back[to, part].astype(F32) + hop[at, k].astype(F32)).astype(BF16)
            sends.send(None, back.at[to, here], shares.at[1 - k, here], rs_in.at[at, 1 - k], (p.s, to))

    def reduce_end(at):
        here = span_of(at)
        total = back[p.t, here].astype(F32)
        for other in (0, 1) if quad else p.planes():
            wait(None, shares.at[other, here], rs_in.at[at, other])
            total = total + shares[other, here].astype(F32)
        reduced[pl.ds(2 * at, 2)] = total.astype(BF16).reshape(2, capp, width)
        for core in range(2):
            to = 2 * at + core
            sends.send(to != p.s, reduced.at[to], returned.at[p.s], rt_in.at[p.s], (to, p.t))

    relay(1)
    phase("chain0")
    wait(None, mate_state, swap_in.at[0])
    wait(None, mate_span, swap_in.at[2])
    forward.step(heads, size, only=p.z == 0)
    line_a.begin(middle=False)
    full_proj[p.s] = proj_ref[...]
    middle = (p.z == side - 1) | (p.z == side)
    if p.chips > 2:
        relay(2, middle)
    turn(1)
    line_a.begin(middle=True)
    line_b.begin()

    phase("near_wait")
    for load in loads:
        load.wait()
    wait(None, rows.at[:, p.mate], dz_in.at[p.mate])
    for at in in_side(sides[0]):
        landed(at >= 0, at)
    phase("near_experts")
    experts_of(sides[0])
    for at in in_side(sides[0]):
        reduce_send(at)
    if p.chips > 2:
        relay(2, ~middle)
    for d in range(3, p.chips):
        relay(d)
    for d in range(2, p.chips):
        turn(d)
    phase("line_a1")
    line_a.step(1)
    if p.chips > 2:
        phase("chain1")
        forward.step(heads, size, only=p.z == 1)
    phase("far_wait")
    for at in in_side(sides[1]):
        landed(at >= 0, at)
    phase("near_turn")
    for at in in_side(sides[0]):
        reduce_turn(at)
    phase("far_experts")
    experts_of(sides[1])
    for at in in_side(sides[1]):
        reduce_send(at)
    phase("line_b1")
    line_b.step(1)
    phase("near_reduce")
    for at in in_side(sides[0]):
        reduce_end(at)

    def weight_grads(k, _):
        at = pl.ds(pl.multiple_of(k * chunk, chunk), chunk)
        in_rows = rows[0].reshape(slots, model)
        dg_ref[at, :] = mm(gate_g[:, at], in_rows, TN).astype(BF16)
        du_ref[at, :] = mm(up_g[:, at], in_rows, TN).astype(BF16)
        dd_ref[at, :] = mm(act[:, at], rows[1].reshape(slots, model), TN).astype(BF16)
        return 0

    phase("wgrads0")
    loops = hidden // chunk
    lax.fori_loop(0, (loops + 1) // 2, weight_grads, 0)
    phase("far_turn")
    for at in in_side(sides[1]):
        reduce_turn(at)
    phase("chain2")
    for d in range(2, p.chips - 1):
        forward.step(heads, size, only=p.z == d)
    phase("line_a2")
    if p.chips > 2:
        line_a.step(2)
    phase("wgrads1")
    if loops > 1:
        lax.fori_loop((loops + 1) // 2, loops, weight_grads, 0)
    phase("far_reduce")
    for at in in_side(sides[1]):
        reduce_end(at)
    returned[p.s] = reduced[p.s]
    phase("line_b2")
    if p.chips > 2:
        line_b.step(2)
    phase("chain3")
    forward.step(heads, size, only=p.z == p.chips - 1)
    forward.finish(heads, size, state_in)
    phase("enter")
    enter_part(groups, y_ref, gate_ref, c_ref, log_ref, state_in, mixer_out, gated)
    all_gated[p.s] = gated[...]
    gather = Line(p, sends, gated, lambda s: all_gated.at[s], gated_in)
    gather.begin()
    phase("line_3")
    for d in range(3, p.chips):
        line_a.step(d)
        line_b.step(d)
    phase("ret_wait")
    for d in range(1, n):
        source = lax.rem(p.s + d, n)
        wait(None, returned.at[source], rt_in.at[source])
    phase("combine")
    stream[:, mine] = (g_ref[:, mine].astype(F32) + mm(picked_ref[...], returned[...].reshape(slots, width))).astype(BF16)
    for other in p.planes():
        sends.send(None, stream.at[:, mine], stream.at[:, mine], st_in.at[p.t], (p.s, other))
    phase("st_wait")
    for other in p.planes():
        wait(None, stream.at[:, cols(other)], st_in.at[other])
    step = max(share, 128)
    part = tokens // m
    split = part % 16 == 0
    some = pl.ds(pl.multiple_of(p.t * part, part), part) if split else pl.ds(0, tokens)

    def columns(j):
        return pl.ds(pl.multiple_of(j * share // step * step, 128), step)

    base = sends.block(n)
    for _, at, ok in p.around():
        for core in range(2):
            to = at * 2 + core
            sends.send(
                ok, stream.at[some, columns(to)], all_stream.at[p.s, some], as_in.at[p.s], (to, p.t), base + to
            )
    sends.send(None, stream.at[some, columns(p.mate)], all_stream.at[p.s, some], as_in.at[p.s], (p.mate, p.t))
    all_stream[p.s, some] = stream[some, columns(p.s)]
    phase("line_end")
    line_a.end()
    line_b.end()
    phase("gated_grad")
    gated_grad[...] = mm(stream[...], full_proj[...].reshape(model, v_ref.shape[1]))
    gate_part(groups, gated_grad, mixer_out, gate_ref, c_ref, log_ref, grad_gate_ref, mixer_grad, own_grad)
    phase("swap_b")
    backward = Chain(
        p, sends, 1, own_grad, mate_grad, span, mate_span, carry_b, onward_b, bwd_in, swap_in.at[1]
    )
    backward.exchange()
    gather.step(1)
    wait(None, mate_grad, swap_in.at[1])
    backward.step(heads, size, only=p.z == p.chips - 1)
    phase("inner")
    inner_part(
        groups, v_ref, b_ref, c_ref, steps_ref, log_ref, logt_ref, mixer_grad, state_in,
        out_keys_ref, in_part_ref, x_part_ref, base_ref,
    )
    phase("back1")
    backward.step(heads, size, only=p.z == p.chips - 2)
    phase("as_wait")
    for d in range(1, n):
        source = lax.rem(p.s + d, n)
        wait(None, all_stream.at[source, some], as_in.at[source])
    if split:
        for other in p.planes():
            sends.send(None, all_stream.at[:, some], all_stream.at[:, some], ag_in.at[p.t], (p.s, other))
    for d in range(2, p.chips):
        phase(f"gather{d}")
        gather.step(d)
        phase(f"back{d}")
        backward.step(heads, size, only=p.z == p.chips - 1 - d)
    phase("back_fin")
    backward.finish(heads, size, after_ref)
    phase("gather_end")
    gather.end()
    phase("ag_wait")
    if split:
        for other in p.planes():
            theirs = pl.ds(pl.multiple_of(other * part, part), part)
            wait(None, all_stream.at[:, theirs], ag_in.at[other])
    phase("fin")
    sends.finish()
    phase(None)


def last_kernel(
    cfg,
    dg_in, du_in, dd_in, grad_gate_in, out_keys_in, in_part_ref, x_part_ref, base_ref, log_ref,
    state_in, after_ref, all_stream, all_gated, steps_ref, v_ref, b_ref, rates_ref,
    dg_out, du_out, dd_out, proj_grad_ref, values_ref, grad_gate_ref, in_keys_ref, out_keys_ref, steps_grad_ref,
    sums, sems,
):
    n, m, groups, capp, width, share = cfg
    phase = Phase()
    phase("proj")
    outs = [
        pltpu.make_async_copy(src, dst, sems.at[k])
        for k, (src, dst) in enumerate(((dg_in, dg_out), (du_in, du_out), (dd_in, dd_out)))
    ]
    for copy in outs:
        copy.start()
    tokens = all_stream.shape[0] * all_stream.shape[1]
    step = all_stream.shape[2]
    grad = mm(all_stream[...].reshape(tokens, step), all_gated[...].reshape(tokens, all_gated.shape[2]), TN)
    if step == share:
        proj_grad_ref[...] = grad
    else:
        sums[...] = grad
        off = pl.multiple_of(lax.rem(lax.axis_index("sp"), step // share) * share, share)
        proj_grad_ref[...] = sums[pl.ds(off, share), :]
    phase("pass")
    grad_gate_ref[...] = grad_gate_in[...]
    out_keys_ref[...] = out_keys_in[...]
    phase("outer")
    outer_part(
        groups, after_ref, state_in, v_ref, b_ref, steps_ref, log_ref, rates_ref,
        in_part_ref, x_part_ref, base_ref, values_ref, in_keys_ref, steps_grad_ref,
    )
    phase("stores")
    for copy in outs:
        copy.wait()
    phase(None)


def body(
    mix_values, mix_gate, input_keys, output_keys, step_sizes, decay_rates, out_proj, expert_inputs,
    stream_grad, routes, route_weights, gate_proj, up_proj, down_proj,
):
    tokens, inner = mix_values.shape
    model = stream_grad.shape[1]
    top = routes.shape[1]
    n, m = lax.axis_size("sp"), lax.axis_size("tp")
    experts = gate_proj.shape[0] * n
    cap = 3 * tokens * top // (2 * experts)
    capp = -(-cap // 16) * 16
    slots = n * capp
    heads = step_sizes.shape[1]
    groups = input_keys.shape[1] // NSTATE
    width = model // m
    hidden = gate_proj.shape[1]
    share = model // n
    chips = n // 2
    step = max(share, 128)
    rates = decay_rates.reshape(1, heads)
    cfg = (n, m, groups, capp, width, share)
    vm, anyw = pl.BlockSpec(memory_space=pltpu.VMEM), pl.BlockSpec(memory_space=pl.ANY)
    keys_shape = input_keys.shape
    weight = (hidden, model)
    dma = pltpu.SemaphoreType.DMA
    sent = (
        2 * n + 6 + 4 + chips * (m + 2) + 2 * (5 + 4 * (chips - 1)) + 3 + 4 * (chips - 1)
        + chips * max(4, m - 1) + 2 * chips + 2 * (m - 1)
    )
    small = (
        mix_values, mix_gate, input_keys, output_keys, step_sizes.T, rates, out_proj, expert_inputs,
        stream_grad, routes.T, route_weights.T,
    )
    first = pl.pallas_call(
        first_kernel,
        out_shape=out((8, 128), F32),
        out_specs=vm,
        cost_estimate=pl.CostEstimate(flops=10**10, bytes_accessed=4096, transcendentals=0),
        compiler_params=pltpu.CompilerParams(vmem_limit_bytes=2**20),
    )()
    mids = pl.pallas_call(
        functools.partial(comm_kernel, cfg),
        out_shape=[
            out(weight, BF16), out(weight, BF16), out(weight, BF16),
            out((tokens, inner), BF16), out(keys_shape, BF16), out(keys_shape, F32),
            out((tokens, inner), F32), out((tokens, heads), F32), out((tokens, heads), F32),
            out((inner, NSTATE), BF16), out((inner, NSTATE), F32),
            out((n, tokens, step), BF16), out((n, tokens, inner), BF16), out((tokens, heads), F32),
        ],
        in_specs=[vm] * 11 + [anyw] * 4,
        out_specs=[vm] * 14,
        scratch_shapes=[
            pltpu.VMEM(weight, BF16), pltpu.VMEM(weight, BF16), pltpu.VMEM(weight, BF16),
            pltpu.VMEM((heads, tokens), F32),
            pltpu.VMEM((tokens, inner), F32), pltpu.VMEM((tokens, inner), F32), pltpu.VMEM((tokens, inner), BF16),
            pltpu.VMEM((inner, NSTATE), BF16), pltpu.VMEM((inner, NSTATE), BF16),
            pltpu.VMEM((inner, NSTATE), BF16), pltpu.VMEM((inner, NSTATE), BF16),
            pltpu.VMEM((8, 128), F32), pltpu.VMEM((8, 128), F32),
            pltpu.VMEM((2, inner // 2, NSTATE), BF16), pltpu.VMEM((inner // 2, NSTATE), BF16),
            pltpu.VMEM((2, inner // 2, NSTATE), BF16), pltpu.VMEM((inner // 2, NSTATE), BF16),
            pltpu.VMEM((tokens, inner), F32), pltpu.VMEM((tokens, inner), F32),
            pltpu.VMEM((tokens, slots), BF16),
            pltpu.VMEM((2, n, capp, width), BF16),
            pltpu.VMEM((2, capp, model), BF16),
            pltpu.VMEM((2, n, capp, model), BF16),
            pltpu.VMEM((slots, hidden), BF16), pltpu.VMEM((slots, hidden), BF16), pltpu.VMEM((slots, hidden), BF16),
            pltpu.VMEM((m, slots, width), BF16), pltpu.VMEM((2 if m == 4 else m, slots, width), BF16),
            pltpu.VMEM((chips, 2, capp, width), BF16),
            pltpu.VMEM((n, capp, width), BF16), pltpu.VMEM((n, capp, width), BF16),
            pltpu.VMEM((tokens, model), BF16),
            pltpu.VMEM((n,) + out_proj.shape, BF16),
            dma((sent,)), dma((3,)), dma((n,)), dma((chips, m)), dma((chips, 2)), dma((chips, 2)), dma((chips, m)),
            dma((n,)), dma((m,)), dma((n,)), dma((m,)),
            dma((n,)), dma((n,)), dma((n,)), dma((2,)), dma((2,)), dma((3,)),
        ],
        cost_estimate=pl.CostEstimate(flops=10**10, bytes_accessed=3 * 10**7, transcendentals=0),
        compiler_params=pltpu.CompilerParams(
            collective_id=0, has_side_effects=True, vmem_limit_bytes=40 * 2**20
        ),
    )(
        *small, first,
        gate_proj.reshape(weight), up_proj.reshape(weight), down_proj.reshape(weight),
    )
    log = mids[8]
    outs = pl.pallas_call(
        functools.partial(last_kernel, cfg),
        out_shape=[
            out(weight, BF16), out(weight, BF16), out(weight, BF16),
            out((share, inner), F32), out((tokens, inner), BF16), out((tokens, inner), BF16),
            out(keys_shape, BF16), out(keys_shape, BF16), out((heads, tokens), F32),
        ],
        in_specs=[vm] * 17,
        out_specs=[anyw] * 3 + [vm] * 6,
        scratch_shapes=[pltpu.VMEM((step, inner), F32), dma((3,))],
        cost_estimate=pl.CostEstimate(flops=10**9, bytes_accessed=2 * 10**7, transcendentals=0),
        compiler_params=pltpu.CompilerParams(vmem_limit_bytes=24 * 2**20),
    )(*mids, mix_values, input_keys, rates)
    shape = gate_proj.shape
    return tuple(o.reshape(shape) for o in outs[:3]) + tuple(outs[3:-1]) + (outs[-1].T,)


def solution(mesh):
    return jax.shard_map(
        body,
        mesh=mesh,
        in_specs=(
            P("sp", "tp"), P("sp", "tp"), P("sp", "tp"), P("sp", "tp"), P("sp", "tp"), P("tp"),
            P("sp", "tp"), P("sp", None), P("sp", None), P("sp", None), P("sp", None),
            P("sp", "tp", None), P("sp", "tp", None), P("sp", "tp", None),
        ),
        out_specs=(
            P("sp", "tp", None), P("sp", "tp", None), P("sp", "tp", None),
            P("sp", "tp"), P("sp", "tp"), P("sp", "tp"), P("sp", "tp"), P("sp", "tp"), P("sp", "tp"),
        ),
        check_vma=False,
    )
```

```python
import functools

import jax
import jax.numpy as jnp
from jax import lax
from jax.experimental import pallas as pl
from jax.experimental.pallas import tpu as pltpu
from jax.sharding import PartitionSpec as P

NSTATE = 128
CLAMP_LIMIT = 7.0
SIGMOID_SCALE = 1.702
HIGHEST = lax.Precision.HIGHEST
F32 = jnp.float32
BF16 = jnp.bfloat16
NN = (((1,), (0,)), ((), ()))
NT = (((1,), (1,)), ((), ()))
TN = (((0,), (0,)), ((), ()))
MESH = pl.DeviceIdType.MESH
VMEM_BYTES = 67043328


def mm(a, b, dims=NN):
    return lax.dot_general(a, b, dims, preferred_element_type=F32)


def mm_exact(a, b, dims=NN):
    return lax.dot_general(a, b, dims, precision=HIGHEST, preferred_element_type=F32)


def grid_of(rows, cols):
    return (
        lax.broadcasted_iota(jnp.int32, (rows, cols), 0),
        lax.broadcasted_iota(jnp.int32, (rows, cols), 1),
    )


def spread(heads, size):
    at, col = grid_of(heads, heads * size)
    return ((col >= at * size) & (col < (at + 1) * size)).astype(F32)


def fold(heads, size):
    col, at = grid_of(heads * size, heads)
    return ((col >= at * size) & (col < (at + 1) * size)).astype(F32)


def padded(a):
    *lead, rows, cols = a.shape
    count = -(-rows // 8) * 8 * (-(-cols // 128) * 128)
    for size in lead:
        count *= size
    return count * a.dtype.itemsize


def out(shape, dtype):
    return jax.ShapeDtypeStruct(shape, dtype)


def mixing_of(log_ref, logt_ref, h):
    length = log_ref.shape[0]
    row, col = grid_of(length, length)
    gap = log_ref[:, h : h + 1] - logt_ref[h : h + 1, :]
    return jnp.where(row >= col, jnp.exp(jnp.minimum(gap, 0.0)), 0.0)


def local_part(groups, v_ref, b_ref, c_ref, steps_ref, log_ref, logt_ref, y_ref, state_ref):
    heads = steps_ref.shape[1]
    per, size = heads // groups, v_ref.shape[1] // heads
    wide = per * size
    length = v_ref.shape[0]
    expand = spread(heads, size)
    to_end = jnp.exp(log_ref[length - 1 :, :] - log_ref[...])
    x = v_ref[...].astype(F32) * mm_exact(steps_ref[...], expand)
    xe = (x * mm_exact(to_end, expand)).astype(BF16)
    x = x.astype(BF16)
    for g in range(groups):
        keys = b_ref[:, g * NSTATE : (g + 1) * NSTATE]
        scores = mm(c_ref[:, g * NSTATE : (g + 1) * NSTATE], keys, NT)
        parts = []
        for r in range(per):
            h = g * per + r
            att = (scores * mixing_of(log_ref, logt_ref, h)).astype(BF16)
            parts.append(mm(att, x[:, h * size : (h + 1) * size]))
        y_ref[:, g * wide : (g + 1) * wide] = jnp.concatenate(parts, axis=1)
        state_ref[g * wide : (g + 1) * wide, :] = mm(
            xe[:, g * wide : (g + 1) * wide], keys, TN
        ).astype(BF16)


def enter_part(groups, y_ref, gate_ref, c_ref, log_ref, state_ref, out_ref, gated_ref):
    heads = log_ref.shape[1]
    per, size = heads // groups, y_ref.shape[1] // heads
    wide = per * size
    decay = mm_exact(jnp.exp(log_ref[...]), spread(heads, size))
    for g in range(groups):
        at = slice(g * wide, (g + 1) * wide)
        entered = mm(c_ref[:, g * NSTATE : (g + 1) * NSTATE], state_ref[at, :], NT) * decay[:, at]
        mixed = y_ref[:, at] + entered
        out_ref[:, at] = mixed
        gate = gate_ref[:, at].astype(F32)
        gated_ref[:, at] = (mixed * gate * jax.nn.sigmoid(gate)).astype(BF16)


def gate_part(groups, grad_ref, out_ref, gate_ref, c_ref, log_ref, gate_grad_ref, mixer_ref, state_ref):
    heads = log_ref.shape[1]
    wide = grad_ref.shape[1] // groups
    decay = mm_exact(jnp.exp(log_ref[...]), spread(heads, grad_ref.shape[1] // heads))
    for g in range(groups):
        at = slice(g * wide, (g + 1) * wide)
        gate = gate_ref[:, at].astype(F32)
        sig = jax.nn.sigmoid(gate)
        grad = grad_ref[:, at]
        gate_grad_ref[:, at] = (grad * out_ref[:, at] * sig * (1.0 + gate * (1.0 - sig))).astype(BF16)
        mixer = grad * gate * sig
        mixer_ref[:, at] = mixer
        keys = c_ref[:, g * NSTATE : (g + 1) * NSTATE]
        state_ref[at, :] = mm((mixer * decay[:, at]).astype(BF16), keys, TN).astype(BF16)


def inner_part(
    groups, v_ref, b_ref, c_ref, steps_ref, log_ref, logt_ref, mixer_ref, state_ref,
    out_keys_ref, in_part_ref, x_part_ref, base_ref,
):
    heads = steps_ref.shape[1]
    per, size = heads // groups, v_ref.shape[1] // heads
    wide = per * size
    length = v_ref.shape[0]
    row, col = grid_of(length, length)
    later = (row <= col).astype(BF16)
    expand = spread(heads, size)
    mixer = mixer_ref[...]
    decayed = mixer * mm_exact(jnp.exp(log_ref[...]), expand)
    decayed_low = decayed.astype(BF16)
    mixer = mixer.astype(BF16)
    x = (v_ref[...].astype(F32) * mm_exact(steps_ref[...], expand)).astype(BF16)
    entering = []
    _, head_at = grid_of(length, heads)
    pairs = jnp.zeros((length, heads), F32)
    for g in range(groups):
        at = slice(g * wide, (g + 1) * wide)
        keys_in = b_ref[:, g * NSTATE : (g + 1) * NSTATE]
        keys_out = c_ref[:, g * NSTATE : (g + 1) * NSTATE]
        scores = mm(keys_out, keys_in, NT)
        score_grad = jnp.zeros((length, length), F32)
        parts = []
        for r in range(per):
            h = g * per + r
            here = slice(h * size, (h + 1) * size)
            mixing = mixing_of(log_ref, logt_ref, h)
            att = scores * mixing
            att_grad = mm(mixer[:, here], x[:, here], NT)
            parts.append(mm(att.astype(BF16), mixer[:, here], TN))
            score_grad = score_grad + att_grad * mixing
            after = mm(later, (att_grad * att).astype(BF16))
            crossing = jnp.sum(jnp.where(col < row, after, 0.0), axis=1, keepdims=True)
            pairs = pairs + jnp.where(head_at == h, crossing, 0.0)
        x_part_ref[:, at] = jnp.concatenate(parts, axis=1)
        score_grad = score_grad.astype(BF16)
        state = state_ref[at, :]
        out_keys_ref[:, g * NSTATE : (g + 1) * NSTATE] = (
            mm(score_grad, keys_in) + mm(decayed_low[:, at], state)
        ).astype(BF16)
        in_part_ref[:, g * NSTATE : (g + 1) * NSTATE] = mm(score_grad, keys_out, TN)
        entering.append(decayed[:, at] * mm(keys_out, state, NT))
    entering = jnp.concatenate(entering, axis=1)
    sums = mm_exact(entering, fold(heads, size))
    base_ref[...] = pairs + mm_exact((row <= col).astype(F32), sums)


def outer_part(
    groups, after_ref, state_ref, v_ref, b_ref, steps_ref, log_ref, rates_ref,
    in_part_ref, x_part_ref, base_ref, values_ref, in_keys_ref, steps_grad_ref,
):
    heads = steps_ref.shape[1]
    per, size = heads // groups, v_ref.shape[1] // heads
    wide = per * size
    length = v_ref.shape[0]
    row, col = grid_of(length, length)
    expand = spread(heads, size)
    last = log_ref[length - 1 :, :]
    steps = mm_exact(steps_ref[...], expand)
    to_end = mm_exact(jnp.exp(last - log_ref[...]), expand)
    values = v_ref[...].astype(F32)
    xe = values * steps * to_end
    xe_low = xe.astype(BF16)
    leaving, direct = [], []
    _, head_at = grid_of(1, heads)
    passing = jnp.zeros((1, heads), F32)
    for g in range(groups):
        at = slice(g * wide, (g + 1) * wide)
        keys_in = b_ref[:, g * NSTATE : (g + 1) * NSTATE]
        for r in range(per):
            h = g * per + r
            here = slice(h * size, (h + 1) * size)
            both = after_ref[here, :] * state_ref[here, :].astype(F32)
            both = jnp.sum(jnp.sum(both, axis=0, keepdims=True), axis=1, keepdims=True)
            passing = passing + jnp.where(head_at == h, both, 0.0)
        after = after_ref[at, :].astype(BF16)
        reached = mm(keys_in, after, NT)
        x_grad = x_part_ref[:, at] + reached * to_end[:, at]
        values_ref[:, at] = (x_grad * steps[:, at]).astype(BF16)
        in_keys_ref[:, g * NSTATE : (g + 1) * NSTATE] = (
            in_part_ref[:, g * NSTATE : (g + 1) * NSTATE] + mm(xe_low[:, at], after)
        ).astype(BF16)
        leaving.append(reached * xe[:, at])
        direct.append(x_grad * values[:, at])
    gather = fold(heads, size)
    leaving = mm_exact(jnp.concatenate(leaving, axis=1), gather)
    direct = mm_exact(jnp.concatenate(direct, axis=1), gather)
    crossing = base_ref[...] + mm_exact((col < row).astype(F32), leaving) + jnp.exp(last) * passing
    steps_grad_ref[...] = (direct - rates_ref[...] * crossing).T


class Phase:
    def __init__(self):
        self.scope = None

    def __call__(self, name):
        if self.scope is not None:
            self.scope.__exit__(None, None, None)
        self.scope = name and jax.named_scope(name)
        if self.scope is not None:
            self.scope.__enter__()


class Sends:
    def __init__(self, sems):
        self.sems, self.used, self.open = sems, 0, []
        self.always = lax.axis_index("tp") >= 0

    def block(self, count):
        self.used += count
        return self.used - count

    def copy(self, src, dst, landed, to, at):
        sem = self.sems.at[self.block(1) if at is None else at]
        return pltpu.make_async_remote_copy(
            src_ref=src, dst_ref=dst, send_sem=sem, recv_sem=landed,
            device_id=to, device_id_type=MESH,
        )

    def send(self, cond, src, dst, landed, to, at=None):
        copy = self.copy(src, dst, landed, to, at)
        when(self.always if cond is None else cond, copy.start)
        self.open.append((cond, copy))

    def finish(self):
        assert self.used <= self.sems.shape[0]
        for cond, copy in self.open:
            when(cond, copy.wait_send)


def when(cond, action):
    if cond is None:
        action()
    else:
        pl.when(cond)(action)


def both(a, b):
    return a if b is None else b if a is None else a & b


class Place:
    def __init__(self, n, m):
        self.n, self.m, self.chips = n, m, n // 2
        self.s, self.t = lax.axis_index("sp"), lax.axis_index("tp")
        self.z, self.c = self.s // 2, lax.rem(self.s, 2)
        self.mate = self.z * 2 + 1 - self.c

    def order(self):
        return [1] + list(range(self.chips - 1, 1, -1))

    def around(self):
        for d in self.order():
            for sign in (1, -1):
                at = self.z + sign * d
                yield d, at, (at >= 0) & (at < self.chips)

    def wait(self, cond, ref, sem):
        copy = pltpu.make_async_remote_copy(
            src_ref=ref, dst_ref=ref, send_sem=sem, recv_sem=sem,
            device_id=(self.mate, self.t), device_id_type=MESH,
        )
        when(cond, copy.wait_recv)

    def planes(self):
        for d in range(1, self.m):
            yield lax.rem(self.t + d, self.m)


class Line:
    def __init__(self, place, sends, own, block, landed):
        self.p, self.sends, self.own, self.block, self.landed = place, sends, own, block, landed
        self.at = sends.block(2 * place.chips + 2)

    def put(self, cond, src, owner, to, at):
        self.sends.send(cond, src, self.block(owner), self.landed.at[owner], (to, self.p.t), at)

    def begin(self, middle=None):
        p = self.p
        down, up = p.z > 0, p.z < p.chips - 1
        down_middle, up_middle = p.z == p.chips // 2, p.z == p.chips // 2 - 1
        if middle is not None:
            down = down & (down_middle if middle else ~down_middle)
            up = up & (up_middle if middle else ~up_middle)
        onward, across = self.at, self.at + p.chips
        self.put(down, self.own, p.s, p.s - 2, onward + 2 * p.chips)
        self.put(up, self.own, p.s, p.s + 2, onward + 2 * p.chips + 1)
        if not middle:
            self.put(None, self.own, p.s, p.mate, across + p.z)

    def step(self, d, only=None):
        p = self.p
        onward, across = self.at, self.at + p.chips
        below, above = p.s - 2 * d, p.s + 2 * d
        from_below, from_above = both(p.z >= d, only), both(p.z + d < p.chips, only)
        p.wait(from_below, self.block(below), self.landed.at[below])
        if d < p.chips - 1:
            self.put(from_below & (p.z < p.chips - 1), self.block(below), below, p.s + 2, onward + p.z - d)
        self.put(from_below, self.block(below), below, p.mate, across + p.z - d)
        p.wait(from_above, self.block(above), self.landed.at[above])
        if d < p.chips - 1:
            self.put(from_above & (p.z > 0), self.block(above), above, p.s - 2, onward + p.z + d)
        self.put(from_above, self.block(above), above, p.mate, across + p.z + d)

    def end(self):
        for k in range(self.p.chips):
            owner = 2 * k + 1 - self.p.c
            self.p.wait(None, self.block(owner), self.landed.at[owner])


class Chain:
    def __init__(self, place, sends, first, own, mates, span, mate_span, carry, onward, landed, swapped):
        self.p, self.sends, self.first = place, sends, first
        self.own, self.mates, self.span, self.mate_span = own, mates, span, mate_span
        self.carry, self.onward, self.landed, self.swapped = carry, onward, landed, swapped
        self.starts = place.z == (0 if first == 0 else place.chips - 1)
        self.stops = place.z == (place.chips - 1 if first == 0 else 0)
        self.next = place.s + (2 if first == 0 else -2)
        self.pieces = landed.shape[0] // 2
        self.at = sends.block(2 * self.pieces)

    def exchange(self):
        p = self.p
        self.sends.send(None, self.own, self.mates, self.swapped, (p.mate, p.t))

    def chunk(self, core, k):
        rows = self.carry.shape[1] // self.pieces
        return self.carry.at[core, pl.ds(k * rows, rows)]

    def step(self, heads, size, only=None):
        p, c = self.p, self.p.c
        half = heads // 2
        rows = half * size
        some = half // self.pieces

        def zero():
            self.carry[...] = jnp.zeros(self.carry.shape, self.carry.dtype)

        when(both(self.starts, only), zero)
        mine, other = jnp.exp(self.span[0:1, :]), jnp.exp(self.mate_span[0:1, :])
        near = c == self.first
        go = both(~self.stops, only)
        for k in range(self.pieces):
            piece = self.chunk(c, k)
            self.p.wait(both(~self.starts, only), piece, self.landed.at[k])

            def advance():
                for r in range(k * some, (k + 1) * some):
                    at = pl.ds(pl.multiple_of(c * rows + r * size, size), size)
                    low, high = slice(r, r + 1), slice(half + r, half + r + 1)
                    w_mine = jnp.where(c == 0, mine[:, low], mine[:, high])
                    w_other = jnp.where(c == 0, other[:, low], other[:, high])
                    own, mate = self.own[at, :].astype(F32), self.mates[at, :].astype(F32)
                    carried = self.carry[c, r * size : (r + 1) * size, :].astype(F32)
                    a = jnp.where(near, w_mine, w_other) * carried + jnp.where(near, own, mate)
                    b = jnp.where(near, w_other, w_mine) * a + jnp.where(near, mate, own)
                    self.onward[r * size : (r + 1) * size, :] = b.astype(BF16)

            when(go, advance)
            self.sends.send(
                go, self.onward.at[pl.ds(k * some * size, some * size)], piece, self.landed.at[k],
                (self.next, p.t), self.at + self.pieces + k,
            )
            self.sends.send(
                both(~self.starts, only), piece, piece, self.landed.at[self.pieces + k], (p.mate, p.t), self.at + k
            )

    def finish(self, heads, size, target):
        p = self.p
        half = heads // 2
        rows = half * size
        for k in range(self.pieces):
            self.p.wait(~self.starts, self.chunk(1 - p.c, k), self.landed.at[self.pieces + k])
        other = jnp.exp(self.mate_span[0:1, :])
        near = p.c == self.first
        for h in range(heads):
            at = slice(h * size, (h + 1) * size)
            inside = slice((h % half) * size, (h % half + 1) * size)
            carried = self.carry[h // half, inside, :].astype(F32)
            through = other[:, h : h + 1] * carried + self.mates[at, :].astype(F32)
            target[at, :] = jnp.where(near, carried, through).astype(target.dtype)


def first_kernel(out_ref):
    out_ref[...] = jnp.zeros(out_ref.shape, out_ref.dtype)


def comm_kernel(
    cfg,
    v_ref, gate_ref, b_ref, c_ref, steps_t_ref, rates_ref, proj_ref, x_ref, g_ref, routes_t_ref, weights_t_ref,
    first_ref, wg_hbm, wu_hbm, wd_hbm,
    dg_ref, du_ref, dd_ref, grad_gate_ref, out_keys_ref, in_part_ref, x_part_ref, base_ref, log_ref,
    state_in, after_ref, proj_grad_ref, steps_ref,
    all_stream, all_gated, sums, wg, wu, wd, logt_ref, y_ref, mixer_out, gated, own_state, mate_state, own_grad, mate_grad,
    span, mate_span, carry_f, onward_f, carry_b, onward_b, gated_grad, mixer_grad,
    picked_ref, parts, local, rows, act, gate_g, up_g, back, shares, hop, reduced, returned, stream, full_proj,
    send_sems, load_sems, dz_in, dp_in, dq_in, hop_in, rs_in, rt_in, st_in, as_in, ag_in,
    low_in, high_in, gated_in, fwd_in, bwd_in, swap_in,
):
    n, m, groups, capp, width, share = cfg
    p = Place(n, m)
    wait = p.wait
    sends = Sends(send_sems)
    phase = Phase()
    top, tokens = routes_t_ref.shape
    heads = steps_t_ref.shape[0]
    size = v_ref.shape[1] // heads
    slots = n * capp
    model = x_ref.shape[1]
    hidden = wg.shape[0]
    quad = m == 4
    by_x, by_y, across = p.t + 1 - 2 * lax.rem(p.t, 2), lax.rem(p.t + 2, 4), 3 - p.t

    lanes = 2 if quad else m
    targets = list(enumerate((by_x, by_y) if quad else p.planes()))

    def cols(t):
        return pl.ds(pl.multiple_of(t * width, 128), width)

    mine = cols(p.t)

    phase("barrier")
    pairs = ((wg_hbm, wg), (wu_hbm, wu), (wd_hbm, wd))
    loads = [pltpu.make_async_copy(src, dst, load_sems.at[k]) for k, (src, dst) in enumerate(pairs)]
    for load in loads:
        load.start()
    barrier = pltpu.get_barrier_semaphore()
    for d in range(1, n):
        pl.semaphore_signal(barrier, inc=1, device_id=(lax.rem(p.s + d, n), p.t), device_id_type=MESH)
    for other in p.planes():
        pl.semaphore_signal(barrier, inc=1, device_id=(p.s, other), device_id_type=MESH)
    half_rows = proj_ref.shape[0] // 2
    low, high = pl.ds(0, half_rows), pl.ds(half_rows, half_rows)
    line_a = Line(p, sends, proj_ref.at[low], lambda s: full_proj.at[s, low], low_in)
    line_b = Line(p, sends, proj_ref.at[high], lambda s: full_proj.at[s, high], high_in)

    phase("slots")
    routes = routes_t_ref[...].T
    weights = weights_t_ref[...].T
    row, col = grid_of(tokens, tokens)
    _, expert = grid_of(tokens, n)
    _, slot = grid_of(tokens, slots)
    _, near = grid_of(tokens, 2 * capp)
    near = jnp.where(near < capp, p.s * capp + near, p.mate * capp + near - capp)
    hits = [expert == routes[:, k : k + 1] for k in range(top)]
    named = sum(hit.astype(F32) for hit in hits)
    before = mm((row > col).astype(BF16), named.astype(BF16))
    every = jnp.zeros((tokens, slots), F32)
    every_near = jnp.zeros((tokens, 2 * capp), F32)
    grads = jnp.zeros((slots, width), F32)
    g_part = g_ref[:, mine].astype(F32)
    nears = []
    for k in range(top):
        rank = jnp.sum(jnp.where(hits[k], before, 0.0), axis=1, keepdims=True).astype(jnp.int32)
        at = routes[:, k : k + 1] * capp + rank
        chosen = (slot == at).astype(F32)
        chosen_near = (near == at).astype(F32)
        every, every_near = every + chosen, every_near + chosen_near
        weight = weights[:, k : k + 1]
        grads = grads + mm(chosen.astype(BF16), (g_part * weight).astype(BF16), TN)
        nears.append((chosen_near.astype(BF16), weight))
    picked = every.astype(BF16)
    parts[0] = mm(picked, x_ref[:, mine], TN).astype(BF16).reshape(n, capp, width)
    parts[1] = grads.astype(BF16).reshape(n, capp, width)
    phase("dispatch")
    pl.semaphore_wait(barrier, n + m - 2)
    base = sends.block(n)
    for _, at, ok in p.around():
        for core in range(2):
            to = at * 2 + core
            sends.send(ok, parts.at[:, to], rows.at[:, p.s, :, mine], dz_in.at[p.s], (to, p.t), base + to)
    phase("near")
    picked_ref[...] = picked
    x_near = mm(every_near.astype(BF16), x_ref[...], TN).astype(BF16)
    grads_near = sum(
        mm(chosen, (g_ref[...].astype(F32) * weight).astype(BF16), TN) for chosen, weight in nears
    ).astype(BF16)
    local[0] = x_near[capp:]
    local[1] = grads_near[capp:]
    sends.send(None, local, rows.at[:, p.s], dz_in.at[p.s], (p.mate, p.t))
    rows[0, p.s] = x_near[:capp]
    rows[1, p.s] = grads_near[:capp]

    phase("local")
    steps_ref[...] = steps_t_ref[...].T
    log = mm_exact((row >= col).astype(F32), -steps_ref[...] * rates_ref[...])
    log_ref[...] = log
    logt_ref[...] = log.T
    span[...] = jnp.zeros(span.shape, F32)
    span[0:1, 0:heads] = log[tokens - 1 :, :]
    local_part(groups, v_ref, b_ref, c_ref, steps_ref, log_ref, logt_ref, y_ref, own_state)
    forward = Chain(
        p, sends, 0, own_state, mate_state, span, mate_span, carry_f, onward_f, fwd_in, swap_in.at[0]
    )
    forward.exchange()
    sends.send(None, span, mate_span, swap_in.at[2], (p.mate, p.t))

    def pair_of(at, t):
        return rows.at[:, pl.ds(2 * at, 2), :, cols(t)]

    relay_base, turn_base = sends.block(p.chips * lanes), sends.block(p.chips * 2)

    def relay(d, only=None):
        phase(f"relay{d}")
        for sign in (1, -1):
            at = p.z + sign * d
            ok = both((at >= 0) & (at < p.chips), only)
            for core in range(2):
                source = at * 2 + core
                wait(ok, rows.at[:, source, :, mine], dz_in.at[source])
            block = pair_of(at, p.t)
            for lane, other in targets:
                sends.send(
                    ok, block, block, dp_in.at[at, lane if quad else p.t], (p.s, other),
                    relay_base + at * lanes + (lane if quad else other),
                )

    def turn(d):
        if not quad:
            return
        phase(f"turn{d}")
        for sign in (1, -1):
            at = p.z + sign * d
            ok = (at >= 0) & (at < p.chips)
            for k, (source, to) in enumerate(((by_x, by_y), (by_y, by_x))):
                wait(ok, pair_of(at, source), dp_in.at[at, k])
                block = rows.at[k, pl.ds(2 * at, 2), :, cols(source)]
                sends.send(ok, block, block, dq_in.at[at, k], (p.s, to), turn_base + at * 2 + k)

    side = p.chips // 2

    def landed(ok, at):
        ok = ok & (at != p.z)
        if quad:
            for k in range(2):
                wait(ok, rows.at[k, pl.ds(2 * at, 2), :, cols(across)], dq_in.at[at, k])
        else:
            for other in p.planes():
                wait(ok, pair_of(at, other), dp_in.at[at, other])

    chunk = min(256, hidden)
    half = slots // 2
    flip = p.z // side
    sides = (flip, 1 - flip)
    pair = 2 * capp

    def in_side(side_at):
        return [(side_at * side + k) for k in range(side)]

    def experts_of(side_at):
        sources = pl.ds(side_at * (n // 2), n // 2)
        here = pl.ds(pl.multiple_of(side_at * half, half), half)

        def experts(k, _):
            at = pl.ds(pl.multiple_of(k * chunk, chunk), chunk)
            in_rows = rows[0, sources].reshape(half, model)
            gate_pre = mm(in_rows, wg[at, :], NT)
            up_pre = mm(in_rows, wu[at, :], NT)
            act_grad = mm(rows[1, sources].reshape(half, model), wd[at, :], NT)
            gate_clamped = jnp.minimum(gate_pre, CLAMP_LIMIT)
            up_clamped = jnp.clip(up_pre, -CLAMP_LIMIT, CLAMP_LIMIT) + 1.0
            sig = jax.nn.sigmoid(SIGMOID_SCALE * gate_clamped)
            swish = gate_clamped * sig
            act[here, at] = (up_clamped * swish).astype(BF16)
            gate_g[here, at] = jnp.where(
                gate_pre < CLAMP_LIMIT,
                act_grad * up_clamped * sig * (1.0 + SIGMOID_SCALE * gate_clamped * (1.0 - sig)),
                0.0,
            ).astype(BF16)
            up_g[here, at] = jnp.where(jnp.abs(up_pre) < CLAMP_LIMIT, act_grad * swish, 0.0).astype(BF16)
            return 0

        lax.fori_loop(0, hidden // chunk, experts, 0)

        def backs(q, _):
            at = cols(q)
            back[q, here] = (mm(gate_g[here, :], wg[:, at]) + mm(up_g[here, :], wu[:, at])).astype(BF16)
            return 0

        lax.fori_loop(0, m, backs, 0)

    def span_of(at):
        return pl.ds(pl.multiple_of(at * pair, pair), pair)

    def halves_of(at):
        return [pl.ds(pl.multiple_of(at * pair + k * capp, capp), capp) for k in range(2)]

    def reduce_send(at):
        if quad:
            first, second = halves_of(at)
            sends.send(None, back.at[across, first], hop.at[at, 0], hop_in.at[at, 0], (p.s, by_x))
            sends.send(None, back.at[across, second], hop.at[at, 1], hop_in.at[at, 1], (p.s, by_y))
        else:
            here = span_of(at)
            for other in p.planes():
                sends.send(None, back.at[other, here], shares.at[p.t, here], rs_in.at[at, p.t], (p.s, other))

    def reduce_turn(at):
        if not quad:
            return
        here = span_of(at)
        for k, (to, part) in enumerate(zip((by_y, by_x), halves_of(at))):
            wait(None, hop.at[at, k], hop_in.at[at, k])
            back[to, part] = (back[to, part].astype(F32) + hop[at, k].astype(F32)).astype(BF16)
            sends.send(None, back.at[to, here], shares.at[1 - k, here], rs_in.at[at, 1 - k], (p.s, to))

    def reduce_end(at):
        here = span_of(at)
        total = back[p.t, here].astype(F32)
        for other in (0, 1) if quad else p.planes():
            wait(None, shares.at[other, here], rs_in.at[at, other])
            total = total + shares[other, here].astype(F32)
        reduced[pl.ds(2 * at, 2)] = total.astype(BF16).reshape(2, capp, width)
        for core in range(2):
            to = 2 * at + core
            sends.send(to != p.s, reduced.at[to], returned.at[p.s], rt_in.at[p.s], (to, p.t))

    relay(1)
    passes = (p.z > 0) & (p.z < p.chips - 1)
    phase("chain0")
    wait(None, mate_state, swap_in.at[0])
    wait(None, mate_span, swap_in.at[2])
    forward.step(heads, size, only=p.z == 0)
    line_a.begin(middle=False)
    full_proj[p.s] = proj_ref[...]
    late = p.order()[1:]
    turn(1)
    for d in late[:-1]:
        relay(d)
    line_a.begin(middle=True)
    line_b.begin()

    phase("near_wait")
    for load in loads:
        load.wait()
    wait(None, rows.at[:, p.mate], dz_in.at[p.mate])
    for at in in_side(sides[0]):
        landed(at >= 0, at)
    phase("near_experts")
    experts_of(sides[0])
    for at in in_side(sides[0]):
        reduce_send(at)
    for d in late[-1:]:
        relay(d)
    for d in late:
        turn(d)
    if p.chips > 2:
        phase("chain1")
        forward.step(heads, size, only=p.z == 1)
    phase("line_a1")
    line_a.step(1)
    phase("far_wait")
    for at in in_side(sides[1]):
        landed(at >= 0, at)
    phase("near_turn")
    for at in in_side(sides[0]):
        reduce_turn(at)
    phase("far_experts")
    experts_of(sides[1])
    for at in in_side(sides[1]):
        reduce_send(at)
    phase("chain2")
    for d in range(2, p.chips - 1):
        forward.step(heads, size, only=p.z == d)
    phase("line_b1")
    line_b.step(1)
    phase("near_reduce")
    for at in in_side(sides[0]):
        reduce_end(at)

    def weight_grads(k, _):
        at = pl.ds(pl.multiple_of(k * chunk, chunk), chunk)
        in_rows = rows[0].reshape(slots, model)
        dg_ref[at, :] = mm(gate_g[:, at], in_rows, TN).astype(BF16)
        du_ref[at, :] = mm(up_g[:, at], in_rows, TN).astype(BF16)
        dd_ref[at, :] = mm(act[:, at], rows[1].reshape(slots, model), TN).astype(BF16)
        return 0

    phase("wgrads0")
    loops = hidden // chunk
    lax.fori_loop(0, (loops + 1) // 2, weight_grads, 0)
    phase("far_turn")
    for at in in_side(sides[1]):
        reduce_turn(at)
    phase("line_a2")
    if p.chips > 2:
        line_a.step(2)
    phase("wgrads1")
    if loops > 1:
        lax.fori_loop((loops + 1) // 2, loops, weight_grads, 0)
    phase("far_reduce")
    for at in in_side(sides[1]):
        reduce_end(at)
    returned[p.s] = reduced[p.s]
    phase("line_b2")
    if p.chips > 2:
        line_b.step(2, passes)
    phase("chain3")
    forward.step(heads, size, only=p.z == p.chips - 1)
    forward.finish(heads, size, state_in)
    phase("enter")
    enter_part(groups, y_ref, gate_ref, c_ref, log_ref, state_in, mixer_out, gated)
    all_gated[p.s] = gated[...]
    gather = Line(p, sends, gated, lambda s: all_gated.at[s], gated_in)
    gather.begin()
    phase("ret_wait")
    for d in range(1, n):
        source = lax.rem(p.s + d, n)
        wait(None, returned.at[source], rt_in.at[source])
    phase("combine")
    stream[:, mine] = (g_ref[:, mine].astype(F32) + mm(picked_ref[...], returned[...].reshape(slots, width))).astype(BF16)
    for other in p.planes():
        sends.send(None, stream.at[:, mine], stream.at[:, mine], st_in.at[p.t], (p.s, other))
    phase("st_wait")
    for other in p.planes():
        wait(None, stream.at[:, cols(other)], st_in.at[other])
    step = max(share, 128)
    part = tokens // m
    split = part % 16 == 0
    some = pl.ds(pl.multiple_of(p.t * part, part), part) if split else pl.ds(0, tokens)

    def columns(j):
        return pl.ds(pl.multiple_of(j * share // step * step, 128), step)

    base = sends.block(n)
    for _, at, ok in p.around():
        for core in range(2):
            to = at * 2 + core
            sends.send(
                ok, stream.at[some, columns(to)], all_stream.at[p.s, some], as_in.at[p.s], (to, p.t), base + to
            )
    sends.send(None, stream.at[some, columns(p.mate)], all_stream.at[p.s, some], as_in.at[p.s], (p.mate, p.t))
    all_stream[p.s, some] = stream[some, columns(p.s)]
    phase("gather1")
    gather.step(1, passes)
    phase("line_3")
    if p.chips > 2:
        line_b.step(2, ~passes)
    for d in range(3, p.chips):
        line_a.step(d)
        line_b.step(d)
    phase("line_end")
    line_a.end()
    line_b.end()
    phase("gated_grad")
    gated_grad[...] = mm(stream[...], full_proj[...].reshape(model, v_ref.shape[1]))
    gate_part(groups, gated_grad, mixer_out, gate_ref, c_ref, log_ref, grad_gate_ref, mixer_grad, own_grad)
    phase("swap_b")
    backward = Chain(
        p, sends, 1, own_grad, mate_grad, span, mate_span, carry_b, onward_b, bwd_in, swap_in.at[1]
    )
    backward.exchange()
    wait(None, mate_grad, swap_in.at[1])
    backward.step(heads, size, only=p.z == p.chips - 1)
    ag_base = sends.block(m)

    def share_columns(only):
        phase("as_wait")
        for d in range(1, n):
            source = lax.rem(p.s + d, n)
            wait(only, all_stream.at[source, some], as_in.at[source])
        if split:
            for other in p.planes():
                block = all_stream.at[:, some]
                sends.send(only, block, block, ag_in.at[p.t], (p.s, other), ag_base + other)

    share_columns(~passes)
    phase("inner")
    inner_part(
        groups, v_ref, b_ref, c_ref, steps_ref, log_ref, logt_ref, mixer_grad, state_in,
        out_keys_ref, in_part_ref, x_part_ref, base_ref,
    )
    if p.chips > 2:
        phase("gather2")
        gather.step(2, passes)
    phase("gather1")
    gather.step(1, ~passes)
    for d in range(1, p.chips - 1):
        phase(f"back{d}")
        backward.step(heads, size, only=p.z == p.chips - 1 - d)
        if d == 1:
            share_columns(passes)
    if p.chips == 2:
        share_columns(passes)
    for d in range(2, p.chips):
        phase(f"gather{d}")
        gather.step(d, ~passes if d == 2 else None)
    phase("gather_end")
    gather.end()
    phase("ag_wait")
    if split:
        for other in p.planes():
            theirs = pl.ds(pl.multiple_of(other * part, part), part)
            wait(None, all_stream.at[:, theirs], ag_in.at[other])
    phase("proj")
    proj_sum = mm(
        all_stream[...].reshape(n * tokens, step), all_gated[...].reshape(n * tokens, v_ref.shape[1]), TN
    )
    if step == share:
        proj_grad_ref[...] = proj_sum
    else:
        sums[...] = proj_sum
        off = pl.multiple_of(lax.rem(p.s, step // share) * share, share)
        proj_grad_ref[...] = sums[pl.ds(off, share), :]
    phase("back_last")
    backward.step(heads, size, only=p.z == 0)
    phase("back_fin")
    backward.finish(heads, size, after_ref)
    phase("fin")
    sends.finish()
    phase(None)


def last_kernel(
    cfg,
    dg_in, du_in, dd_in, grad_gate_in, out_keys_in, in_part_ref, x_part_ref, base_ref, log_ref,
    state_in, after_ref, proj_grad_in, steps_ref, v_ref, b_ref, rates_ref,
    dg_out, du_out, dd_out, proj_grad_out, values_ref, grad_gate_out, in_keys_ref, out_keys_out, steps_grad_ref,
    sems,
):
    n, m, groups, capp, width, share = cfg
    phase = Phase()
    pairs = (
        (dg_in, dg_out), (du_in, du_out), (dd_in, dd_out), (proj_grad_in, proj_grad_out),
        (grad_gate_in, grad_gate_out), (out_keys_in, out_keys_out),
    )
    outs = [pltpu.make_async_copy(src, dst, sems.at[k]) for k, (src, dst) in enumerate(pairs)]

    def begin():
        for copy in outs:
            copy.start()

    pl.when(lax.axis_index("tp") >= 0)(begin)
    phase("outer")
    outer_part(
        groups, after_ref, state_in, v_ref, b_ref, steps_ref, log_ref, rates_ref,
        in_part_ref, x_part_ref, base_ref, values_ref, in_keys_ref, steps_grad_ref,
    )
    phase("stores")

    def end():
        for copy in outs:
            copy.wait()

    pl.when(lax.axis_index("tp") >= 0)(end)
    phase(None)


def body(
    mix_values, mix_gate, input_keys, output_keys, step_sizes, decay_rates, out_proj, expert_inputs,
    stream_grad, routes, route_weights, gate_proj, up_proj, down_proj,
):
    tokens, inner = mix_values.shape
    model = stream_grad.shape[1]
    top = routes.shape[1]
    n, m = lax.axis_size("sp"), lax.axis_size("tp")
    experts = gate_proj.shape[0] * n
    cap = 3 * tokens * top // (2 * experts)
    capp = -(-cap // 16) * 16
    slots = n * capp
    heads = step_sizes.shape[1]
    groups = input_keys.shape[1] // NSTATE
    width = model // m
    hidden = gate_proj.shape[1]
    share = model // n
    chips = n // 2
    step = max(share, 128)
    rates = decay_rates.reshape(1, heads)
    cfg = (n, m, groups, capp, width, share)
    vm, anyw = pl.BlockSpec(memory_space=pltpu.VMEM), pl.BlockSpec(memory_space=pl.ANY)
    keys_shape = input_keys.shape
    weight = (hidden, model)
    dma = pltpu.SemaphoreType.DMA
    between = 2 if m == 4 else m
    pieces = min(4, heads // 2)
    sent = (
        2 * n + 6 + 4 * pieces + chips * (between + 2) + 3 * (2 * chips + 2)
        + chips * max(4, m - 1) + 2 * chips + 2 * (m - 1)
    )
    small = (
        mix_values, mix_gate, input_keys, output_keys, step_sizes.T, rates, out_proj, expert_inputs,
        stream_grad, routes.T, route_weights.T,
    )
    results = [
        out(weight, BF16), out(weight, BF16), out(weight, BF16),
        out((tokens, inner), BF16), out(keys_shape, BF16), out(keys_shape, F32),
        out((tokens, inner), F32), out((tokens, heads), F32), out((tokens, heads), F32),
        out((inner, NSTATE), BF16), out((inner, NSTATE), F32),
        out((share, inner), F32), out((tokens, heads), F32),
    ]
    room = sum(padded(a) for a in results) + sum(padded(a) for a in small) + 2**18
    first = pl.pallas_call(
        first_kernel,
        out_shape=out((8, 128), F32),
        out_specs=vm,
        cost_estimate=pl.CostEstimate(flops=10**10, bytes_accessed=4096, transcendentals=0),
        compiler_params=pltpu.CompilerParams(vmem_limit_bytes=2**20),
    )()
    mids = pl.pallas_call(
        functools.partial(comm_kernel, cfg),
        out_shape=results,
        in_specs=[vm] * 11 + [anyw] * 4,
        out_specs=[vm] * 13,
        scratch_shapes=[
            pltpu.VMEM((n, tokens, step), BF16), pltpu.VMEM((n, tokens, inner), BF16), pltpu.VMEM((step, inner), F32),
            pltpu.VMEM(weight, BF16), pltpu.VMEM(weight, BF16), pltpu.VMEM(weight, BF16),
            pltpu.VMEM((heads, tokens), F32),
            pltpu.VMEM((tokens, inner), F32), pltpu.VMEM((tokens, inner), F32), pltpu.VMEM((tokens, inner), BF16),
            pltpu.VMEM((inner, NSTATE), BF16), pltpu.VMEM((inner, NSTATE), BF16),
            pltpu.VMEM((inner, NSTATE), BF16), pltpu.VMEM((inner, NSTATE), BF16),
            pltpu.VMEM((8, 128), F32), pltpu.VMEM((8, 128), F32),
            pltpu.VMEM((2, inner // 2, NSTATE), BF16), pltpu.VMEM((inner // 2, NSTATE), BF16),
            pltpu.VMEM((2, inner // 2, NSTATE), BF16), pltpu.VMEM((inner // 2, NSTATE), BF16),
            pltpu.VMEM((tokens, inner), F32), pltpu.VMEM((tokens, inner), F32),
            pltpu.VMEM((tokens, slots), BF16),
            pltpu.VMEM((2, n, capp, width), BF16),
            pltpu.VMEM((2, capp, model), BF16),
            pltpu.VMEM((2, n, capp, model), BF16),
            pltpu.VMEM((slots, hidden), BF16), pltpu.VMEM((slots, hidden), BF16), pltpu.VMEM((slots, hidden), BF16),
            pltpu.VMEM((m, slots, width), BF16), pltpu.VMEM((2 if m == 4 else m, slots, width), BF16),
            pltpu.VMEM((chips, 2, capp, width), BF16),
            pltpu.VMEM((n, capp, width), BF16), pltpu.VMEM((n, capp, width), BF16),
            pltpu.VMEM((tokens, model), BF16),
            pltpu.VMEM((n,) + out_proj.shape, BF16),
            dma((sent,)), dma((3,)), dma((n,)), dma((chips, between)), dma((chips, 2)), dma((chips, 2)), dma((chips, between)),
            dma((n,)), dma((m,)), dma((n,)), dma((m,)),
            dma((n,)), dma((n,)), dma((n,)), dma((2 * pieces,)), dma((2 * pieces,)), dma((3,)),
        ],
        cost_estimate=pl.CostEstimate(flops=10**10, bytes_accessed=3 * 10**7, transcendentals=0),
        compiler_params=pltpu.CompilerParams(
            collective_id=0, has_side_effects=True, vmem_limit_bytes=42 * 2**20
        ),
    )(
        *small, first,
        gate_proj.reshape(weight), up_proj.reshape(weight), down_proj.reshape(weight),
    )
    log = mids[8]
    outs = pl.pallas_call(
        functools.partial(last_kernel, cfg),
        out_shape=[
            out(weight, BF16), out(weight, BF16), out(weight, BF16),
            out((share, inner), F32), out((tokens, inner), BF16), out((tokens, inner), BF16),
            out(keys_shape, BF16), out(keys_shape, BF16), out((heads, tokens), F32),
        ],
        in_specs=[vm] * 16,
        out_specs=[anyw] * 4 + [vm, anyw, vm, anyw, vm],
        scratch_shapes=[dma((6,))],
        cost_estimate=pl.CostEstimate(flops=10**9, bytes_accessed=2 * 10**7, transcendentals=0),
        compiler_params=pltpu.CompilerParams(vmem_limit_bytes=24 * 2**20),
    )(*mids, mix_values, input_keys, rates)
    shape = gate_proj.shape
    return tuple(o.reshape(shape) for o in outs[:3]) + tuple(outs[3:-1]) + (outs[-1].T,)


def solution(mesh):
    return jax.shard_map(
        body,
        mesh=mesh,
        in_specs=(
            P("sp", "tp"), P("sp", "tp"), P("sp", "tp"), P("sp", "tp"), P("sp", "tp"), P("tp"),
            P("sp", "tp"), P("sp", None), P("sp", None), P("sp", None), P("sp", None),
            P("sp", "tp", None), P("sp", "tp", None), P("sp", "tp", None),
        ),
        out_specs=(
            P("sp", "tp", None), P("sp", "tp", None), P("sp", "tp", None),
            P("sp", "tp"), P("sp", "tp"), P("sp", "tp"), P("sp", "tp"), P("sp", "tp"), P("sp", "tp"),
        ),
        check_vma=False,
    )
```

```python
import functools

import jax
import jax.numpy as jnp
from jax import lax
from jax.experimental import pallas as pl
from jax.experimental.pallas import tpu as pltpu
from jax.sharding import PartitionSpec as P

NSTATE = 128
CLAMP_LIMIT = 7.0
SIGMOID_SCALE = 1.702
HIGHEST = lax.Precision.HIGHEST
F32 = jnp.float32
BF16 = jnp.bfloat16
NN = (((1,), (0,)), ((), ()))
NT = (((1,), (1,)), ((), ()))
TN = (((0,), (0,)), ((), ()))
MESH = pl.DeviceIdType.MESH
VMEM_BYTES = 67043328


def mm(a, b, dims=NN):
    return lax.dot_general(a, b, dims, preferred_element_type=F32)


def mm_exact(a, b, dims=NN):
    return lax.dot_general(a, b, dims, precision=HIGHEST, preferred_element_type=F32)


def grid_of(rows, cols):
    return (
        lax.broadcasted_iota(jnp.int32, (rows, cols), 0),
        lax.broadcasted_iota(jnp.int32, (rows, cols), 1),
    )


def spread(heads, size):
    at, col = grid_of(heads, heads * size)
    return ((col >= at * size) & (col < (at + 1) * size)).astype(F32)


def fold(heads, size):
    col, at = grid_of(heads * size, heads)
    return ((col >= at * size) & (col < (at + 1) * size)).astype(F32)


def padded(a):
    *lead, rows, cols = a.shape
    count = -(-rows // 8) * 8 * (-(-cols // 128) * 128)
    for size in lead:
        count *= size
    return count * a.dtype.itemsize


def out(shape, dtype):
    return jax.ShapeDtypeStruct(shape, dtype)


def mixing_of(log_ref, logt_ref, h):
    length = log_ref.shape[0]
    row, col = grid_of(length, length)
    gap = log_ref[:, h : h + 1] - logt_ref[h : h + 1, :]
    return jnp.where(row >= col, jnp.exp(jnp.minimum(gap, 0.0)), 0.0)


def local_part(groups, v_ref, b_ref, c_ref, steps_ref, log_ref, logt_ref, y_ref, state_ref):
    heads = steps_ref.shape[1]
    per, size = heads // groups, v_ref.shape[1] // heads
    wide = per * size
    length = v_ref.shape[0]
    expand = spread(heads, size)
    to_end = jnp.exp(log_ref[length - 1 :, :] - log_ref[...])
    x = v_ref[...].astype(F32) * mm_exact(steps_ref[...], expand)
    xe = (x * mm_exact(to_end, expand)).astype(BF16)
    x = x.astype(BF16)
    for g in range(groups):
        keys = b_ref[:, g * NSTATE : (g + 1) * NSTATE]
        scores = mm(c_ref[:, g * NSTATE : (g + 1) * NSTATE], keys, NT)
        parts = []
        for r in range(per):
            h = g * per + r
            att = (scores * mixing_of(log_ref, logt_ref, h)).astype(BF16)
            parts.append(mm(att, x[:, h * size : (h + 1) * size]))
        y_ref[:, g * wide : (g + 1) * wide] = jnp.concatenate(parts, axis=1)
        state_ref[g * wide : (g + 1) * wide, :] = mm(
            xe[:, g * wide : (g + 1) * wide], keys, TN
        ).astype(BF16)


def enter_part(groups, y_ref, gate_ref, c_ref, log_ref, state_ref, out_ref, gated_ref):
    heads = log_ref.shape[1]
    per, size = heads // groups, y_ref.shape[1] // heads
    wide = per * size
    decay = mm_exact(jnp.exp(log_ref[...]), spread(heads, size))
    for g in range(groups):
        at = slice(g * wide, (g + 1) * wide)
        entered = mm(c_ref[:, g * NSTATE : (g + 1) * NSTATE], state_ref[at, :], NT) * decay[:, at]
        mixed = y_ref[:, at] + entered
        out_ref[:, at] = mixed
        gate = gate_ref[:, at].astype(F32)
        gated_ref[:, at] = (mixed * gate * jax.nn.sigmoid(gate)).astype(BF16)


def gate_part(groups, grad_ref, out_ref, gate_ref, c_ref, log_ref, gate_grad_ref, mixer_ref, state_ref):
    heads = log_ref.shape[1]
    wide = grad_ref.shape[1] // groups
    decay = mm_exact(jnp.exp(log_ref[...]), spread(heads, grad_ref.shape[1] // heads))
    for g in range(groups):
        at = slice(g * wide, (g + 1) * wide)
        gate = gate_ref[:, at].astype(F32)
        sig = jax.nn.sigmoid(gate)
        grad = grad_ref[:, at]
        gate_grad_ref[:, at] = (grad * out_ref[:, at] * sig * (1.0 + gate * (1.0 - sig))).astype(BF16)
        mixer = grad * gate * sig
        mixer_ref[:, at] = mixer
        keys = c_ref[:, g * NSTATE : (g + 1) * NSTATE]
        state_ref[at, :] = mm((mixer * decay[:, at]).astype(BF16), keys, TN).astype(BF16)


def inner_part(
    groups, v_ref, b_ref, c_ref, steps_ref, log_ref, logt_ref, mixer_ref, state_ref,
    out_keys_ref, in_part_ref, x_part_ref, base_ref,
):
    heads = steps_ref.shape[1]
    per, size = heads // groups, v_ref.shape[1] // heads
    wide = per * size
    length = v_ref.shape[0]
    row, col = grid_of(length, length)
    later = (row <= col).astype(BF16)
    expand = spread(heads, size)
    mixer = mixer_ref[...]
    decayed = mixer * mm_exact(jnp.exp(log_ref[...]), expand)
    decayed_low = decayed.astype(BF16)
    mixer = mixer.astype(BF16)
    x = (v_ref[...].astype(F32) * mm_exact(steps_ref[...], expand)).astype(BF16)
    entering = []
    _, head_at = grid_of(length, heads)
    pairs = jnp.zeros((length, heads), F32)
    for g in range(groups):
        at = slice(g * wide, (g + 1) * wide)
        keys_in = b_ref[:, g * NSTATE : (g + 1) * NSTATE]
        keys_out = c_ref[:, g * NSTATE : (g + 1) * NSTATE]
        scores = mm(keys_out, keys_in, NT)
        score_grad = jnp.zeros((length, length), F32)
        parts = []
        for r in range(per):
            h = g * per + r
            here = slice(h * size, (h + 1) * size)
            mixing = mixing_of(log_ref, logt_ref, h)
            att = scores * mixing
            att_grad = mm(mixer[:, here], x[:, here], NT)
            parts.append(mm(att.astype(BF16), mixer[:, here], TN))
            score_grad = score_grad + att_grad * mixing
            after = mm(later, (att_grad * att).astype(BF16))
            crossing = jnp.sum(jnp.where(col < row, after, 0.0), axis=1, keepdims=True)
            pairs = pairs + jnp.where(head_at == h, crossing, 0.0)
        x_part_ref[:, at] = jnp.concatenate(parts, axis=1)
        score_grad = score_grad.astype(BF16)
        state = state_ref[at, :]
        out_keys_ref[:, g * NSTATE : (g + 1) * NSTATE] = (
            mm(score_grad, keys_in) + mm(decayed_low[:, at], state)
        ).astype(BF16)
        in_part_ref[:, g * NSTATE : (g + 1) * NSTATE] = mm(score_grad, keys_out, TN)
        entering.append(decayed[:, at] * mm(keys_out, state, NT))
    entering = jnp.concatenate(entering, axis=1)
    sums = mm_exact(entering, fold(heads, size))
    base_ref[...] = pairs + mm_exact((row <= col).astype(F32), sums)


def outer_part(
    groups, after_ref, state_ref, v_ref, b_ref, steps_ref, log_ref, rates_ref,
    in_part_ref, x_part_ref, base_ref, values_ref, in_keys_ref, steps_grad_ref,
):
    heads = steps_ref.shape[1]
    per, size = heads // groups, v_ref.shape[1] // heads
    wide = per * size
    length = v_ref.shape[0]
    row, col = grid_of(length, length)
    expand = spread(heads, size)
    last = log_ref[length - 1 :, :]
    steps = mm_exact(steps_ref[...], expand)
    to_end = mm_exact(jnp.exp(last - log_ref[...]), expand)
    values = v_ref[...].astype(F32)
    xe = values * steps * to_end
    xe_low = xe.astype(BF16)
    leaving, direct = [], []
    _, head_at = grid_of(1, heads)
    passing = jnp.zeros((1, heads), F32)
    for g in range(groups):
        at = slice(g * wide, (g + 1) * wide)
        keys_in = b_ref[:, g * NSTATE : (g + 1) * NSTATE]
        for r in range(per):
            h = g * per + r
            here = slice(h * size, (h + 1) * size)
            both = after_ref[here, :] * state_ref[here, :].astype(F32)
            both = jnp.sum(jnp.sum(both, axis=0, keepdims=True), axis=1, keepdims=True)
            passing = passing + jnp.where(head_at == h, both, 0.0)
        after = after_ref[at, :].astype(BF16)
        reached = mm(keys_in, after, NT)
        x_grad = x_part_ref[:, at] + reached * to_end[:, at]
        values_ref[:, at] = (x_grad * steps[:, at]).astype(BF16)
        in_keys_ref[:, g * NSTATE : (g + 1) * NSTATE] = (
            in_part_ref[:, g * NSTATE : (g + 1) * NSTATE] + mm(xe_low[:, at], after)
        ).astype(BF16)
        leaving.append(reached * xe[:, at])
        direct.append(x_grad * values[:, at])
    gather = fold(heads, size)
    leaving = mm_exact(jnp.concatenate(leaving, axis=1), gather)
    direct = mm_exact(jnp.concatenate(direct, axis=1), gather)
    crossing = base_ref[...] + mm_exact((col < row).astype(F32), leaving) + jnp.exp(last) * passing
    steps_grad_ref[...] = (direct - rates_ref[...] * crossing).T


class Phase:
    def __init__(self):
        self.scope = None

    def __call__(self, name):
        if self.scope is not None:
            self.scope.__exit__(None, None, None)
        self.scope = name and jax.named_scope(name)
        if self.scope is not None:
            self.scope.__enter__()


class Sends:
    def __init__(self, sems):
        self.sems, self.used, self.open = sems, 0, []
        self.always = lax.axis_index("tp") >= 0

    def block(self, count):
        self.used += count
        return self.used - count

    def copy(self, src, dst, landed, to, at):
        sem = self.sems.at[self.block(1) if at is None else at]
        return pltpu.make_async_remote_copy(
            src_ref=src, dst_ref=dst, send_sem=sem, recv_sem=landed,
            device_id=to, device_id_type=MESH,
        )

    def send(self, cond, src, dst, landed, to, at=None):
        copy = self.copy(src, dst, landed, to, at)
        when(self.always if cond is None else cond, copy.start)
        self.open.append((cond, copy))

    def finish(self):
        assert self.used <= self.sems.shape[0]
        for cond, copy in self.open:
            when(cond, copy.wait_send)


def when(cond, action):
    if cond is None:
        action()
    else:
        pl.when(cond)(action)


def both(a, b):
    return a if b is None else b if a is None else a & b


class Place:
    def __init__(self, n, m):
        self.n, self.m, self.chips = n, m, n // 2
        self.s, self.t = lax.axis_index("sp"), lax.axis_index("tp")
        self.z, self.c = self.s // 2, lax.rem(self.s, 2)
        self.mate = self.z * 2 + 1 - self.c

    def order(self):
        return [1] + list(range(self.chips - 1, 1, -1))

    def around(self):
        for d in self.order():
            for sign in (1, -1):
                at = self.z + sign * d
                yield d, at, (at >= 0) & (at < self.chips)

    def wait(self, cond, ref, sem):
        copy = pltpu.make_async_remote_copy(
            src_ref=ref, dst_ref=ref, send_sem=sem, recv_sem=sem,
            device_id=(self.mate, self.t), device_id_type=MESH,
        )
        when(cond, copy.wait_recv)

    def planes(self):
        for d in range(1, self.m):
            yield lax.rem(self.t + d, self.m)


class Line:
    def __init__(self, place, sends, own, block, landed):
        self.p, self.sends, self.own, self.block, self.landed = place, sends, own, block, landed
        self.at = sends.block(2 * place.chips + 2)

    def put(self, cond, src, owner, to, at):
        self.sends.send(cond, src, self.block(owner), self.landed.at[owner], (to, self.p.t), at)

    def begin(self, middle=None):
        p = self.p
        down, up = p.z > 0, p.z < p.chips - 1
        down_middle, up_middle = p.z == p.chips // 2, p.z == p.chips // 2 - 1
        if middle is not None:
            down = down & (down_middle if middle else ~down_middle)
            up = up & (up_middle if middle else ~up_middle)
        onward, across = self.at, self.at + p.chips
        self.put(down, self.own, p.s, p.s - 2, onward + 2 * p.chips)
        self.put(up, self.own, p.s, p.s + 2, onward + 2 * p.chips + 1)
        if not middle:
            self.put(None, self.own, p.s, p.mate, across + p.z)

    def step(self, d, only=None):
        p = self.p
        onward, across = self.at, self.at + p.chips
        below, above = p.s - 2 * d, p.s + 2 * d
        from_below, from_above = both(p.z >= d, only), both(p.z + d < p.chips, only)
        p.wait(from_below, self.block(below), self.landed.at[below])
        if d < p.chips - 1:
            self.put(from_below & (p.z < p.chips - 1), self.block(below), below, p.s + 2, onward + p.z - d)
        self.put(from_below, self.block(below), below, p.mate, across + p.z - d)
        p.wait(from_above, self.block(above), self.landed.at[above])
        if d < p.chips - 1:
            self.put(from_above & (p.z > 0), self.block(above), above, p.s - 2, onward + p.z + d)
        self.put(from_above, self.block(above), above, p.mate, across + p.z + d)

    def end(self):
        for k in range(self.p.chips):
            owner = 2 * k + 1 - self.p.c
            self.p.wait(None, self.block(owner), self.landed.at[owner])


class Chain:
    def __init__(self, place, sends, first, own, mates, span, mate_span, carry, onward, landed, swapped):
        self.p, self.sends, self.first = place, sends, first
        self.own, self.mates, self.span, self.mate_span = own, mates, span, mate_span
        self.carry, self.onward, self.landed, self.swapped = carry, onward, landed, swapped
        self.starts = place.z == (0 if first == 0 else place.chips - 1)
        self.stops = place.z == (place.chips - 1 if first == 0 else 0)
        self.next = place.s + (2 if first == 0 else -2)
        self.pieces = landed.shape[0] // 2
        self.at = sends.block(2 * self.pieces)

    def exchange(self):
        p = self.p
        self.sends.send(None, self.own, self.mates, self.swapped, (p.mate, p.t))

    def chunk(self, core, k):
        rows = self.carry.shape[1] // self.pieces
        return self.carry.at[core, pl.ds(k * rows, rows)]

    def step(self, heads, size, only=None):
        p, c = self.p, self.p.c
        half = heads // 2
        rows = half * size
        some = half // self.pieces

        def zero():
            self.carry[...] = jnp.zeros(self.carry.shape, self.carry.dtype)

        when(both(self.starts, only), zero)
        mine, other = jnp.exp(self.span[0:1, :]), jnp.exp(self.mate_span[0:1, :])
        near = c == self.first
        go = both(~self.stops, only)
        for k in range(self.pieces):
            piece = self.chunk(c, k)
            self.p.wait(both(~self.starts, only), piece, self.landed.at[k])

            def advance():
                for r in range(k * some, (k + 1) * some):
                    at = pl.ds(pl.multiple_of(c * rows + r * size, size), size)
                    low, high = slice(r, r + 1), slice(half + r, half + r + 1)
                    w_mine = jnp.where(c == 0, mine[:, low], mine[:, high])
                    w_other = jnp.where(c == 0, other[:, low], other[:, high])
                    own, mate = self.own[at, :].astype(F32), self.mates[at, :].astype(F32)
                    carried = self.carry[c, r * size : (r + 1) * size, :].astype(F32)
                    a = jnp.where(near, w_mine, w_other) * carried + jnp.where(near, own, mate)
                    b = jnp.where(near, w_other, w_mine) * a + jnp.where(near, mate, own)
                    self.onward[r * size : (r + 1) * size, :] = b.astype(BF16)

            when(go, advance)
            self.sends.send(
                go, self.onward.at[pl.ds(k * some * size, some * size)], piece, self.landed.at[k],
                (self.next, p.t), self.at + self.pieces + k,
            )
            self.sends.send(
                both(~self.starts, only), piece, piece, self.landed.at[self.pieces + k], (p.mate, p.t), self.at + k
            )

    def finish(self, heads, size, target):
        p = self.p
        half = heads // 2
        rows = half * size
        for k in range(self.pieces):
            self.p.wait(~self.starts, self.chunk(1 - p.c, k), self.landed.at[self.pieces + k])
        other = jnp.exp(self.mate_span[0:1, :])
        near = p.c == self.first
        for h in range(heads):
            at = slice(h * size, (h + 1) * size)
            inside = slice((h % half) * size, (h % half + 1) * size)
            carried = self.carry[h // half, inside, :].astype(F32)
            through = other[:, h : h + 1] * carried + self.mates[at, :].astype(F32)
            target[at, :] = jnp.where(near, carried, through).astype(target.dtype)


def first_kernel(out_ref):
    out_ref[...] = jnp.zeros(out_ref.shape, out_ref.dtype)


def comm_kernel(
    cfg,
    v_ref, gate_ref, b_ref, c_ref, steps_t_ref, rates_ref, proj_ref, x_ref, g_ref, routes_t_ref, weights_t_ref,
    first_ref, wg_hbm, wu_hbm, wd_hbm,
    dg_ref, du_ref, dd_ref, grad_gate_ref, out_keys_ref, in_part_ref, x_part_ref, base_ref, log_ref,
    state_in, after_ref, proj_grad_ref, steps_ref,
    all_stream, all_gated, sums, wg, wu, wd, logt_ref, y_ref, mixer_out, gated, own_state, mate_state, own_grad, mate_grad,
    span, mate_span, carry_f, onward_f, carry_b, onward_b, gated_grad, mixer_grad,
    picked_ref, parts, local, rows, act, gate_g, up_g, back, shares, hop, reduced, returned, stream, full_proj,
    send_sems, load_sems, dz_in, dp_in, dq_in, hop_in, rs_in, rt_in, st_in, as_in, ag_in,
    low_in, high_in, gated_in, fwd_in, bwd_in, swap_in,
):
    n, m, groups, capp, width, share = cfg
    p = Place(n, m)
    wait = p.wait
    sends = Sends(send_sems)
    phase = Phase()
    top, tokens = routes_t_ref.shape
    heads = steps_t_ref.shape[0]
    size = v_ref.shape[1] // heads
    slots = n * capp
    model = x_ref.shape[1]
    hidden = wg.shape[0]
    quad = m == 4
    by_x, by_y, across = p.t + 1 - 2 * lax.rem(p.t, 2), lax.rem(p.t + 2, 4), 3 - p.t

    lanes = 2 if quad else m
    targets = list(enumerate((by_x, by_y) if quad else p.planes()))

    def cols(t):
        return pl.ds(pl.multiple_of(t * width, 128), width)

    mine = cols(p.t)

    phase("barrier")
    pairs = ((wg_hbm, wg), (wu_hbm, wu), (wd_hbm, wd))
    loads = [pltpu.make_async_copy(src, dst, load_sems.at[k]) for k, (src, dst) in enumerate(pairs)]
    for load in loads:
        load.start()
    barrier = pltpu.get_barrier_semaphore()
    for d in range(1, n):
        pl.semaphore_signal(barrier, inc=1, device_id=(lax.rem(p.s + d, n), p.t), device_id_type=MESH)
    for other in p.planes():
        pl.semaphore_signal(barrier, inc=1, device_id=(p.s, other), device_id_type=MESH)
    half_rows = proj_ref.shape[0] // 2
    low, high = pl.ds(0, half_rows), pl.ds(half_rows, half_rows)
    line_a = Line(p, sends, proj_ref.at[low], lambda s: full_proj.at[s, low], low_in)
    line_b = Line(p, sends, proj_ref.at[high], lambda s: full_proj.at[s, high], high_in)

    phase("slots")
    routes = routes_t_ref[...].T
    weights = weights_t_ref[...].T
    row, col = grid_of(tokens, tokens)
    _, expert = grid_of(tokens, n)
    _, slot = grid_of(tokens, slots)
    _, near = grid_of(tokens, 2 * capp)
    near = jnp.where(near < capp, p.s * capp + near, p.mate * capp + near - capp)
    hits = [expert == routes[:, k : k + 1] for k in range(top)]
    named = sum(hit.astype(F32) for hit in hits)
    before = mm((row > col).astype(BF16), named.astype(BF16))
    every = jnp.zeros((tokens, slots), F32)
    every_near = jnp.zeros((tokens, 2 * capp), F32)
    grads = jnp.zeros((slots, width), F32)
    g_part = g_ref[:, mine].astype(F32)
    nears = []
    for k in range(top):
        rank = jnp.sum(jnp.where(hits[k], before, 0.0), axis=1, keepdims=True).astype(jnp.int32)
        at = routes[:, k : k + 1] * capp + rank
        chosen = (slot == at).astype(F32)
        chosen_near = (near == at).astype(F32)
        every, every_near = every + chosen, every_near + chosen_near
        weight = weights[:, k : k + 1]
        grads = grads + mm(chosen.astype(BF16), (g_part * weight).astype(BF16), TN)
        nears.append((chosen_near.astype(BF16), weight))
    picked = every.astype(BF16)
    parts[0] = mm(picked, x_ref[:, mine], TN).astype(BF16).reshape(n, capp, width)
    parts[1] = grads.astype(BF16).reshape(n, capp, width)
    phase("dispatch")
    pl.semaphore_wait(barrier, n + m - 2)
    base = sends.block(n)
    for _, at, ok in p.around():
        for core in range(2):
            to = at * 2 + lax.rem(core + p.c, 2)
            sends.send(ok, parts.at[:, to], rows.at[:, p.s, :, mine], dz_in.at[p.s], (to, p.t), base + to)
    phase("near")
    picked_ref[...] = picked
    x_near = mm(every_near.astype(BF16), x_ref[...], TN).astype(BF16)
    grads_near = sum(
        mm(chosen, (g_ref[...].astype(F32) * weight).astype(BF16), TN) for chosen, weight in nears
    ).astype(BF16)
    local[0] = x_near[capp:]
    local[1] = grads_near[capp:]
    sends.send(None, local, rows.at[:, p.s], dz_in.at[p.s], (p.mate, p.t))
    rows[0, p.s] = x_near[:capp]
    rows[1, p.s] = grads_near[:capp]

    phase("local")
    steps_ref[...] = steps_t_ref[...].T
    log = mm_exact((row >= col).astype(F32), -steps_ref[...] * rates_ref[...])
    log_ref[...] = log
    logt_ref[...] = log.T
    span[...] = jnp.zeros(span.shape, F32)
    span[0:1, 0:heads] = log[tokens - 1 :, :]
    local_part(groups, v_ref, b_ref, c_ref, steps_ref, log_ref, logt_ref, y_ref, own_state)
    forward = Chain(
        p, sends, 0, own_state, mate_state, span, mate_span, carry_f, onward_f, fwd_in, swap_in.at[0]
    )
    forward.exchange()
    sends.send(None, span, mate_span, swap_in.at[2], (p.mate, p.t))

    def pair_of(at, t):
        return rows.at[:, pl.ds(2 * at, 2), :, cols(t)]

    relay_base, turn_base = sends.block(p.chips * lanes), sends.block(p.chips * 2)

    def relay(d, only=None):
        phase(f"relay{d}")
        for sign in (1, -1):
            at = p.z + sign * d
            ok = both((at >= 0) & (at < p.chips), only)
            for core in range(2):
                source = at * 2 + core
                wait(ok, rows.at[:, source, :, mine], dz_in.at[source])
            block = pair_of(at, p.t)
            for lane, other in targets:
                sends.send(
                    ok, block, block, dp_in.at[at, lane if quad else p.t], (p.s, other),
                    relay_base + at * lanes + (lane if quad else other),
                )

    def turn(d):
        if not quad:
            return
        phase(f"turn{d}")
        for sign in (1, -1):
            at = p.z + sign * d
            ok = (at >= 0) & (at < p.chips)
            for k, (source, to) in enumerate(((by_x, by_y), (by_y, by_x))):
                wait(ok, pair_of(at, source), dp_in.at[at, k])
                block = rows.at[k, pl.ds(2 * at, 2), :, cols(source)]
                sends.send(ok, block, block, dq_in.at[at, k], (p.s, to), turn_base + at * 2 + k)

    side = p.chips // 2

    def landed(ok, at):
        ok = ok & (at != p.z)
        if quad:
            for k in range(2):
                wait(ok, rows.at[k, pl.ds(2 * at, 2), :, cols(across)], dq_in.at[at, k])
        else:
            for other in p.planes():
                wait(ok, pair_of(at, other), dp_in.at[at, other])

    chunk = min(256, hidden)
    half = slots // 2
    flip = p.z // side
    sides = (flip, 1 - flip)
    pair = 2 * capp

    def in_side(side_at):
        return [(side_at * side + k) for k in range(side)]

    def experts_of(side_at):
        sources = pl.ds(side_at * (n // 2), n // 2)
        here = pl.ds(pl.multiple_of(side_at * half, half), half)

        def experts(k, _):
            at = pl.ds(pl.multiple_of(k * chunk, chunk), chunk)
            in_rows = rows[0, sources].reshape(half, model)
            gate_pre = mm(in_rows, wg[at, :], NT)
            up_pre = mm(in_rows, wu[at, :], NT)
            act_grad = mm(rows[1, sources].reshape(half, model), wd[at, :], NT)
            gate_clamped = jnp.minimum(gate_pre, CLAMP_LIMIT)
            up_clamped = jnp.clip(up_pre, -CLAMP_LIMIT, CLAMP_LIMIT) + 1.0
            sig = jax.nn.sigmoid(SIGMOID_SCALE * gate_clamped)
            swish = gate_clamped * sig
            act[here, at] = (up_clamped * swish).astype(BF16)
            gate_g[here, at] = jnp.where(
                gate_pre < CLAMP_LIMIT,
                act_grad * up_clamped * sig * (1.0 + SIGMOID_SCALE * gate_clamped * (1.0 - sig)),
                0.0,
            ).astype(BF16)
            up_g[here, at] = jnp.where(jnp.abs(up_pre) < CLAMP_LIMIT, act_grad * swish, 0.0).astype(BF16)
            return 0

        lax.fori_loop(0, hidden // chunk, experts, 0)

        def backs(q, _):
            at = cols(q)
            back[q, here] = (mm(gate_g[here, :], wg[:, at]) + mm(up_g[here, :], wu[:, at])).astype(BF16)
            return 0

        lax.fori_loop(0, m, backs, 0)

    def span_of(at):
        return pl.ds(pl.multiple_of(at * pair, pair), pair)

    def halves_of(at):
        return [pl.ds(pl.multiple_of(at * pair + k * capp, capp), capp) for k in range(2)]

    def reduce_send(at):
        if quad:
            first, second = halves_of(at)
            sends.send(None, back.at[across, first], hop.at[at, 0], hop_in.at[at, 0], (p.s, by_x))
            sends.send(None, back.at[across, second], hop.at[at, 1], hop_in.at[at, 1], (p.s, by_y))
        else:
            here = span_of(at)
            for other in p.planes():
                sends.send(None, back.at[other, here], shares.at[p.t, here], rs_in.at[at, p.t], (p.s, other))

    def reduce_turn(at):
        if not quad:
            return
        here = span_of(at)
        for k, (to, part) in enumerate(zip((by_y, by_x), halves_of(at))):
            wait(None, hop.at[at, k], hop_in.at[at, k])
            back[to, part] = (back[to, part].astype(F32) + hop[at, k].astype(F32)).astype(BF16)
            sends.send(None, back.at[to, here], shares.at[1 - k, here], rs_in.at[at, 1 - k], (p.s, to))

    def reduce_end(at):
        here = span_of(at)
        total = back[p.t, here].astype(F32)
        for other in (0, 1) if quad else p.planes():
            wait(None, shares.at[other, here], rs_in.at[at, other])
            total = total + shares[other, here].astype(F32)
        reduced[pl.ds(2 * at, 2)] = total.astype(BF16).reshape(2, capp, width)
        for core in range(2):
            to = 2 * at + core
            sends.send(to != p.s, reduced.at[to], returned.at[p.s], rt_in.at[p.s], (to, p.t))

    relay(1)
    passes = (p.z > 0) & (p.z < p.chips - 1)
    phase("chain0")
    wait(None, mate_state, swap_in.at[0])
    wait(None, mate_span, swap_in.at[2])
    forward.step(heads, size, only=p.z == 0)
    line_a.begin(middle=False)
    full_proj[p.s] = proj_ref[...]
    late = p.order()[1:]
    turn(1)
    for d in late[:-1]:
        relay(d)
    line_a.begin(middle=True)
    line_b.begin()

    phase("near_wait")
    for load in loads:
        load.wait()
    wait(None, rows.at[:, p.mate], dz_in.at[p.mate])
    for at in in_side(sides[0]):
        landed(at >= 0, at)
    phase("near_experts")
    experts_of(sides[0])
    for at in in_side(sides[0]):
        reduce_send(at)
    for d in late[-1:]:
        relay(d)
    for d in late:
        turn(d)
    if p.chips > 2:
        phase("chain1")
        forward.step(heads, size, only=p.z == 1)
    phase("line_a1")
    line_a.step(1)
    phase("far_wait")
    for at in in_side(sides[1]):
        landed(at >= 0, at)
    phase("near_turn")
    for at in in_side(sides[0]):
        reduce_turn(at)
    phase("far_experts")
    experts_of(sides[1])
    for at in in_side(sides[1]):
        reduce_send(at)
    phase("chain2")
    for d in range(2, p.chips - 1):
        forward.step(heads, size, only=p.z == d)
    phase("line_b1")
    line_b.step(1)
    phase("near_reduce")
    for at in in_side(sides[0]):
        reduce_end(at)

    def weight_grads(k, _):
        at = pl.ds(pl.multiple_of(k * chunk, chunk), chunk)
        in_rows = rows[0].reshape(slots, model)
        dg_ref[at, :] = mm(gate_g[:, at], in_rows, TN).astype(BF16)
        du_ref[at, :] = mm(up_g[:, at], in_rows, TN).astype(BF16)
        dd_ref[at, :] = mm(act[:, at], rows[1].reshape(slots, model), TN).astype(BF16)
        return 0

    phase("wgrads0")
    loops = hidden // chunk
    lax.fori_loop(0, (loops + 1) // 2, weight_grads, 0)
    phase("far_turn")
    for at in in_side(sides[1]):
        reduce_turn(at)
    phase("line_a2")
    if p.chips > 2:
        line_a.step(2)
    phase("wgrads1")
    if loops > 1:
        lax.fori_loop((loops + 1) // 2, loops, weight_grads, 0)
    phase("far_reduce")
    for at in in_side(sides[1]):
        reduce_end(at)
    returned[p.s] = reduced[p.s]
    phase("line_b2")
    if p.chips > 2:
        line_b.step(2, passes)
    phase("chain3")
    forward.step(heads, size, only=p.z == p.chips - 1)
    forward.finish(heads, size, state_in)
    phase("enter")
    enter_part(groups, y_ref, gate_ref, c_ref, log_ref, state_in, mixer_out, gated)
    all_gated[p.s] = gated[...]
    gather = Line(p, sends, gated, lambda s: all_gated.at[s], gated_in)
    gather.begin()
    phase("ret_wait")
    for d in range(1, n):
        source = lax.rem(p.s + d, n)
        wait(None, returned.at[source], rt_in.at[source])
    phase("combine")
    stream[:, mine] = (g_ref[:, mine].astype(F32) + mm(picked_ref[...], returned[...].reshape(slots, width))).astype(BF16)
    for other in p.planes():
        sends.send(None, stream.at[:, mine], stream.at[:, mine], st_in.at[p.t], (p.s, other))
    phase("st_wait")
    for other in p.planes():
        wait(None, stream.at[:, cols(other)], st_in.at[other])
    step = max(share, 128)
    part = tokens // m
    split = part % 16 == 0
    some = pl.ds(pl.multiple_of(p.t * part, part), part) if split else pl.ds(0, tokens)

    def columns(j):
        return pl.ds(pl.multiple_of(j * share // step * step, 128), step)

    base = sends.block(n)
    for _, at, ok in p.around():
        for core in range(2):
            to = at * 2 + core
            sends.send(
                ok, stream.at[some, columns(to)], all_stream.at[p.s, some], as_in.at[p.s], (to, p.t), base + to
            )
    sends.send(None, stream.at[some, columns(p.mate)], all_stream.at[p.s, some], as_in.at[p.s], (p.mate, p.t))
    all_stream[p.s, some] = stream[some, columns(p.s)]
    phase("gather1")
    gather.step(1, passes)
    phase("line_3")
    if p.chips > 2:
        line_b.step(2, ~passes)
    for d in range(3, p.chips):
        line_a.step(d)
        line_b.step(d)
    phase("line_end")
    line_a.end()
    line_b.end()
    phase("gated_grad")
    gated_grad[...] = mm(stream[...], full_proj[...].reshape(model, v_ref.shape[1]))
    gate_part(groups, gated_grad, mixer_out, gate_ref, c_ref, log_ref, grad_gate_ref, mixer_grad, own_grad)
    phase("swap_b")
    backward = Chain(
        p, sends, 1, own_grad, mate_grad, span, mate_span, carry_b, onward_b, bwd_in, swap_in.at[1]
    )
    backward.exchange()
    wait(None, mate_grad, swap_in.at[1])
    backward.step(heads, size, only=p.z == p.chips - 1)
    ag_base = sends.block(m)

    def share_columns(only):
        phase("as_wait")
        for d in range(1, n):
            source = lax.rem(p.s + d, n)
            wait(only, all_stream.at[source, some], as_in.at[source])
        if split:
            for other in p.planes():
                block = all_stream.at[:, some]
                sends.send(only, block, block, ag_in.at[p.t], (p.s, other), ag_base + other)

    share_columns(~passes)
    phase("inner")
    inner_part(
        groups, v_ref, b_ref, c_ref, steps_ref, log_ref, logt_ref, mixer_grad, state_in,
        out_keys_ref, in_part_ref, x_part_ref, base_ref,
    )
    if p.chips > 2:
        phase("gather2")
        gather.step(2, passes)
    phase("gather1")
    gather.step(1, ~passes)
    for d in range(1, p.chips - 1):
        phase(f"back{d}")
        backward.step(heads, size, only=p.z == p.chips - 1 - d)
        if d == 1:
            share_columns(passes)
    if p.chips == 2:
        share_columns(passes)
    for d in range(2, p.chips):
        phase(f"gather{d}")
        gather.step(d, ~passes if d == 2 else None)
    phase("gather_end")
    gather.end()
    phase("ag_wait")
    if split:
        for other in p.planes():
            theirs = pl.ds(pl.multiple_of(other * part, part), part)
            wait(None, all_stream.at[:, theirs], ag_in.at[other])
    phase("proj")
    proj_sum = mm(
        all_stream[...].reshape(n * tokens, step), all_gated[...].reshape(n * tokens, v_ref.shape[1]), TN
    )
    if step == share:
        proj_grad_ref[...] = proj_sum
    else:
        sums[...] = proj_sum
        off = pl.multiple_of(lax.rem(p.s, step // share) * share, share)
        proj_grad_ref[...] = sums[pl.ds(off, share), :]
    phase("back_last")
    backward.step(heads, size, only=p.z == 0)
    phase("back_fin")
    backward.finish(heads, size, after_ref)
    phase("fin")
    sends.finish()
    phase(None)


def last_kernel(
    cfg,
    dg_in, du_in, dd_in, grad_gate_in, out_keys_in, in_part_ref, x_part_ref, base_ref, log_ref,
    state_in, after_ref, proj_grad_in, steps_ref, v_ref, b_ref, rates_ref,
    dg_out, du_out, dd_out, proj_grad_out, values_ref, grad_gate_out, in_keys_ref, out_keys_out, steps_grad_ref,
    sems,
):
    n, m, groups, capp, width, share = cfg
    phase = Phase()
    pairs = (
        (dg_in, dg_out), (du_in, du_out), (dd_in, dd_out), (proj_grad_in, proj_grad_out),
        (grad_gate_in, grad_gate_out), (out_keys_in, out_keys_out),
    )
    outs = [pltpu.make_async_copy(src, dst, sems.at[k]) for k, (src, dst) in enumerate(pairs)]

    def begin():
        for copy in outs:
            copy.start()

    pl.when(lax.axis_index("tp") >= 0)(begin)
    phase("outer")
    outer_part(
        groups, after_ref, state_in, v_ref, b_ref, steps_ref, log_ref, rates_ref,
        in_part_ref, x_part_ref, base_ref, values_ref, in_keys_ref, steps_grad_ref,
    )
    phase("stores")

    def end():
        for copy in outs:
            copy.wait()

    pl.when(lax.axis_index("tp") >= 0)(end)
    phase(None)


def body(
    mix_values, mix_gate, input_keys, output_keys, step_sizes, decay_rates, out_proj, expert_inputs,
    stream_grad, routes, route_weights, gate_proj, up_proj, down_proj,
):
    tokens, inner = mix_values.shape
    model = stream_grad.shape[1]
    top = routes.shape[1]
    n, m = lax.axis_size("sp"), lax.axis_size("tp")
    experts = gate_proj.shape[0] * n
    cap = 3 * tokens * top // (2 * experts)
    capp = -(-cap // 16) * 16
    slots = n * capp
    heads = step_sizes.shape[1]
    groups = input_keys.shape[1] // NSTATE
    width = model // m
    hidden = gate_proj.shape[1]
    share = model // n
    chips = n // 2
    step = max(share, 128)
    rates = decay_rates.reshape(1, heads)
    cfg = (n, m, groups, capp, width, share)
    vm, anyw = pl.BlockSpec(memory_space=pltpu.VMEM), pl.BlockSpec(memory_space=pl.ANY)
    keys_shape = input_keys.shape
    weight = (hidden, model)
    dma = pltpu.SemaphoreType.DMA
    between = 2 if m == 4 else m
    pieces = min(4, heads // 2)
    sent = (
        2 * n + 6 + 4 * pieces + chips * (between + 2) + 3 * (2 * chips + 2)
        + chips * max(4, m - 1) + 2 * chips + 2 * (m - 1)
    )
    small = (
        mix_values, mix_gate, input_keys, output_keys, step_sizes.T, rates, out_proj, expert_inputs,
        stream_grad, routes.T, route_weights.T,
    )
    results = [
        out(weight, BF16), out(weight, BF16), out(weight, BF16),
        out((tokens, inner), BF16), out(keys_shape, BF16), out(keys_shape, F32),
        out((tokens, inner), F32), out((tokens, heads), F32), out((tokens, heads), F32),
        out((inner, NSTATE), BF16), out((inner, NSTATE), F32),
        out((share, inner), F32), out((tokens, heads), F32),
    ]
    room = sum(padded(a) for a in results) + sum(padded(a) for a in small) + 2**18
    first = pl.pallas_call(
        first_kernel,
        out_shape=out((8, 128), F32),
        out_specs=vm,
        cost_estimate=pl.CostEstimate(flops=10**10, bytes_accessed=4096, transcendentals=0),
        compiler_params=pltpu.CompilerParams(vmem_limit_bytes=2**20),
    )()
    mids = pl.pallas_call(
        functools.partial(comm_kernel, cfg),
        out_shape=results,
        in_specs=[vm] * 11 + [anyw] * 4,
        out_specs=[vm] * 13,
        scratch_shapes=[
            pltpu.VMEM((n, tokens, step), BF16), pltpu.VMEM((n, tokens, inner), BF16), pltpu.VMEM((step, inner), F32),
            pltpu.VMEM(weight, BF16), pltpu.VMEM(weight, BF16), pltpu.VMEM(weight, BF16),
            pltpu.VMEM((heads, tokens), F32),
            pltpu.VMEM((tokens, inner), F32), pltpu.VMEM((tokens, inner), F32), pltpu.VMEM((tokens, inner), BF16),
            pltpu.VMEM((inner, NSTATE), BF16), pltpu.VMEM((inner, NSTATE), BF16),
            pltpu.VMEM((inner, NSTATE), BF16), pltpu.VMEM((inner, NSTATE), BF16),
            pltpu.VMEM((8, 128), F32), pltpu.VMEM((8, 128), F32),
            pltpu.VMEM((2, inner // 2, NSTATE), BF16), pltpu.VMEM((inner // 2, NSTATE), BF16),
            pltpu.VMEM((2, inner // 2, NSTATE), BF16), pltpu.VMEM((inner // 2, NSTATE), BF16),
            pltpu.VMEM((tokens, inner), F32), pltpu.VMEM((tokens, inner), F32),
            pltpu.VMEM((tokens, slots), BF16),
            pltpu.VMEM((2, n, capp, width), BF16),
            pltpu.VMEM((2, capp, model), BF16),
            pltpu.VMEM((2, n, capp, model), BF16),
            pltpu.VMEM((slots, hidden), BF16), pltpu.VMEM((slots, hidden), BF16), pltpu.VMEM((slots, hidden), BF16),
            pltpu.VMEM((m, slots, width), BF16), pltpu.VMEM((2 if m == 4 else m, slots, width), BF16),
            pltpu.VMEM((chips, 2, capp, width), BF16),
            pltpu.VMEM((n, capp, width), BF16), pltpu.VMEM((n, capp, width), BF16),
            pltpu.VMEM((tokens, model), BF16),
            pltpu.VMEM((n,) + out_proj.shape, BF16),
            dma((sent,)), dma((3,)), dma((n,)), dma((chips, between)), dma((chips, 2)), dma((chips, 2)), dma((chips, between)),
            dma((n,)), dma((m,)), dma((n,)), dma((m,)),
            dma((n,)), dma((n,)), dma((n,)), dma((2 * pieces,)), dma((2 * pieces,)), dma((3,)),
        ],
        cost_estimate=pl.CostEstimate(flops=10**10, bytes_accessed=3 * 10**7, transcendentals=0),
        compiler_params=pltpu.CompilerParams(
            collective_id=0, has_side_effects=True, vmem_limit_bytes=42 * 2**20
        ),
    )(
        *small, first,
        gate_proj.reshape(weight), up_proj.reshape(weight), down_proj.reshape(weight),
    )
    log = mids[8]
    outs = pl.pallas_call(
        functools.partial(last_kernel, cfg),
        out_shape=[
            out(weight, BF16), out(weight, BF16), out(weight, BF16),
            out((share, inner), F32), out((tokens, inner), BF16), out((tokens, inner), BF16),
            out(keys_shape, BF16), out(keys_shape, BF16), out((heads, tokens), F32),
        ],
        in_specs=[vm] * 16,
        out_specs=[anyw] * 4 + [vm, anyw, vm, anyw, vm],
        scratch_shapes=[dma((6,))],
        cost_estimate=pl.CostEstimate(flops=10**9, bytes_accessed=2 * 10**7, transcendentals=0),
        compiler_params=pltpu.CompilerParams(vmem_limit_bytes=24 * 2**20),
    )(*mids, mix_values, input_keys, rates)
    shape = gate_proj.shape
    return tuple(o.reshape(shape) for o in outs[:3]) + tuple(outs[3:-1]) + (outs[-1].T,)


def solution(mesh):
    return jax.shard_map(
        body,
        mesh=mesh,
        in_specs=(
            P("sp", "tp"), P("sp", "tp"), P("sp", "tp"), P("sp", "tp"), P("sp", "tp"), P("tp"),
            P("sp", "tp"), P("sp", None), P("sp", None), P("sp", None), P("sp", None),
            P("sp", "tp", None), P("sp", "tp", None), P("sp", "tp", None),
        ),
        out_specs=(
            P("sp", "tp", None), P("sp", "tp", None), P("sp", "tp", None),
            P("sp", "tp"), P("sp", "tp"), P("sp", "tp"), P("sp", "tp"), P("sp", "tp"), P("sp", "tp"),
        ),
        check_vma=False,
    )
```
